32 devices in a mesh: ep: 16 (over z, x, core), tp: 2 (over y).
Axes of the slice: x: 2, y: 2, z: 4, core: 2. Of those that a mesh axis runs over, the one named last changes fastest.
Arguments:
- tokens: bfloat16 [512, 2048], P('ep'), may hold values from -6 to 6
- norm_gain_attn: float32 [2048], replicated, may hold values from 0.1 to 1.9
- w_query: bfloat16 [2048, 2048], P('ep', 'tp'), may hold values from -0.125 to 0.125
- w_key: bfloat16 [2048, 256], P('ep', 'tp'), may hold values from -0.125 to 0.125
- w_value: bfloat16 [2048, 256], P('ep', 'tp'), may hold values from -0.125 to 0.125
- w_forget: bfloat16 [2048, 32], P(None, 'tp'), may hold values from -0.125 to 0.125
- forget_bias: float32 [32], P('tp'), may hold values from -1 to 3
- cache_keys: bfloat16 [512, 256, 1024], P('ep', 'tp'), may hold values from -64 to 64
- cache_values: bfloat16 [512, 256, 1024], P('ep', 'tp'), may hold values from -6 to 6
- cache_logcum: float32 [512, 32, 1024], P('ep', 'tp'), may hold values from -2048 to 0, as said below
- lengths: int32 [512], P('ep'), may hold values from 1 to 1023, as said below
- w_out: bfloat16 [2048, 2048], P('tp'), may hold values from -0.125 to 0.125
- norm_gain_mix: float32 [2048], replicated, may hold values from 0.1 to 1.9
- norm_gain_ffn: float32 [2048], replicated, may hold values from 0.1 to 1.9
- expert_gate: bfloat16 [2048, 16384], P(None, ('ep', 'tp')), may hold values from -0.125 to 0.125
- expert_up: bfloat16 [2048, 16384], P(None, ('ep', 'tp')), may hold values from -0.125 to 0.125
- expert_down: bfloat16 [16384, 2048], P(('ep', 'tp')), may hold values from -0.09375 to 0.09375
- routes: int32 [512, 2], P('ep'), may hold values from 0 to 3, all different within a row; in each aligned block of 32 rows (0 to 31, 32 to 63, ...) at most 32 rows name the same one
- route_weights: float32 [512, 2], P('ep'), may hold values from 0.2 to 1
Outputs:
- layer_out: bfloat16 [512, 2048], P('ep', 'tp')
- new_keys: bfloat16 [512, 256], P('ep', 'tp')
- new_values: bfloat16 [512, 256], P('ep', 'tp')
- new_log_gate: float32 [512, 32], P('ep', 'tp')
The draws below stay inside these ranges and needn't reach their ends.
Inputs may be any that keep to these rules, and one draw needn't show every extreme that they name: `routes`: each row names 2 different experts. Within the rows of one index of ep no expert is named by more than 32 rows, and in every draw some expert is named by exactly 32 rows of some index. `lengths`: some sequence has 1023 cached positions in every draw. `cache_logcum`: never rising along positions (the last dimension).
All inputs are finite; a program needn't handle non-finite values.
Results may differ from the reference program's by a relative error of at most 0.013.
Values may be sent and summed in bfloat16 or wider, within the bound.
A program may use at most 64 MiB of HBM per device.

```python
import math
import jax
import jax.numpy as jnp
import numpy as np
from jax import lax

D = 2048
HEAD_TOTAL = 32
KV_HEADS = 4
HEAD_DIM = 64
FF = 4096
TOP = 2
B_DEV = 32
LENGTH_LIMIT = 1024
SEQUENCE_TOTAL = 512
EXPERTS = 4
CAP = 32
N_TP = 2


def draw_cache_logcum(key, part):
    gathered_keys = jax.random.split(key, 5)
    fast_share = 0.5
    fast_heads = jax.random.uniform(gathered_keys[0], (HEAD_TOTAL,)) < fast_share
    head_rate = jnp.where(fast_heads, 0.1, 0.5 / LENGTH_LIMIT)
    seq_factor = jnp.exp(jax.random.uniform(gathered_keys[1], (SEQUENCE_TOTAL, 1, 1), minval=-0.7, maxval=0.7))
    rough_factor = jnp.exp(jax.random.uniform(gathered_keys[2], (SEQUENCE_TOTAL, LENGTH_LIMIT, HEAD_TOTAL), minval=-0.7, maxval=0.7))
    decode_step_gates = -head_rate[None, None, :] * seq_factor * rough_factor
    spike_positions = jax.random.uniform(gathered_keys[3], (SEQUENCE_TOTAL, LENGTH_LIMIT, 1)) < 2.0 / LENGTH_LIMIT
    spike_penalty = jax.random.uniform(gathered_keys[4], (SEQUENCE_TOTAL, LENGTH_LIMIT, HEAD_TOTAL), minval=0.22, maxval=0.69)
    decode_step_gates = decode_step_gates - jnp.where(spike_positions, spike_penalty, 0.0)
    summed = jnp.cumsum(decode_step_gates, axis=1)
    return jnp.transpose(summed, (0, 2, 1)).astype(jnp.float32)


def draw_cache_keys(key, part):
    gathered_keys = jax.random.split(key, 1)
    shape_full = (SEQUENCE_TOTAL, LENGTH_LIMIT, KV_HEADS * HEAD_DIM)
    result = jnp.clip(jax.random.normal(gathered_keys[0], shape_full), -6.0, 6.0)
    return jnp.transpose(result, (0, 2, 1)).astype(jnp.bfloat16)


def draw_lengths(key, part):
    gathered_keys = jax.random.split(key, 3)
    block_tops = jax.random.randint(gathered_keys[0], (SEQUENCE_TOTAL // B_DEV, 1), LENGTH_LIMIT // 8, LENGTH_LIMIT)
    raw_draws = jax.random.randint(gathered_keys[1], (SEQUENCE_TOTAL // B_DEV, B_DEV), 0, LENGTH_LIMIT)
    seq_lengths = (1 + raw_draws % block_tops).reshape(-1)
    chosen = jax.random.randint(gathered_keys[2], (), 0, SEQUENCE_TOTAL)
    seq_lengths = seq_lengths.at[chosen].set(LENGTH_LIMIT - 1)
    return seq_lengths.astype(jnp.int32)


def block_levels(rng, dims, pieces, least, largest):
    def one(dim, shards_of):
        draws = jax.random.uniform(jax.random.fold_in(jax.random.fold_in(rng, 6), dim), (shards_of,), jnp.float32, least / len(pieces), largest / len(pieces))
        return jnp.repeat(jnp.exp(draws), dims[dim] // shards_of).reshape((-1,) + (1,) * (len(dims) - dim - 1))

    loudness = one(*pieces[0])
    for cut in pieces[1:]:
        loudness = loudness * one(*cut)
    return loudness


def assign_block(rng, own, number, rows, number_of, top, bound, lean):
    ranking = jax.random.permutation(rng, number_of)
    heavy_load, common = shares(number_of, rows * top, bound, lean, True), shares(number_of, rows * top, bound, lean, False)
    places = jnp.arange(number_of)

    def named(sizes, rotation):
        used = int((sizes > 0).sum())
        fixed = max(1, used // 4)
        passed = fixed + (places - fixed + rotation * (used - fixed)) % max(1, number_of - fixed)
        return jnp.zeros((number_of,), jnp.int32).at[ranking[jnp.where(places < fixed, places, passed)]].set(jnp.asarray(sizes, jnp.int32))

    sizes = jnp.where(number % 4 == 0, named(heavy_load, number // 4), named(common, number - number // 4 - 1))
    mixed = jax.random.permutation(jax.random.fold_in(own, 3), number_of)
    donor, receiver = mixed[0:number_of // 2 * 2:2], mixed[1:number_of // 2 * 2:2]
    margin = jnp.minimum(sizes[donor] - 1, bound - sizes[receiver]) // 2
    margin = jnp.where((donor == ranking[0]) | (receiver == ranking[0]) | (sizes[receiver] == 0), 0, jnp.maximum(margin, 0))
    passed = jax.random.randint(jax.random.fold_in(own, 4), (number_of // 2,), 0, 1 << 20) % (margin + 1)
    sizes = sizes.at[donor].add(-passed).at[receiver].add(passed)
    labels = jnp.searchsorted(jnp.cumsum(sizes), jnp.arange(rows * top), side="right").astype(jnp.int32)
    grid = labels.reshape(top, rows).T
    grid = grid[jax.random.permutation(jax.random.fold_in(own, 1), rows)]
    rotation = jax.random.randint(jax.random.fold_in(own, 2), (rows, 1), 0, top)
    return jnp.take_along_axis(grid, (jnp.arange(top)[None, :] + rotation) % top, axis=1)


def shares(count, total, bound, lean, full):
    loads = [(1 << 20) // math.isqrt(rank ** lean) + 1 for rank in range(1, count + 1)]
    largest = bound if full else min(bound, max(-(-total // count), total * loads[0] // sum(loads)))
    least = 1 if total - largest >= count - 1 else 0
    holding, rest = [largest] + [least] * (count - 1), total - largest - least * (count - 1)
    while rest > 0:
        candidates = [i for i in range(1, count) if holding[i] < largest] or [i for i in range(1, count) if holding[i] < bound]
        pool, remaining = sum([loads[i] for i in candidates]), rest
        for i in candidates:
            addition = min(bound - holding[i], max(1, remaining * loads[i] // pool), rest)
            holding[i] = holding[i] + addition
            rest = rest - addition
    return np.array(holding)


def bell_draw(rng, shape, width, most, cuts=(), kind=jnp.bfloat16):
    level = block_levels(rng, shape, cuts, -0.22, 0.18) if cuts else 1.0
    values = jax.random.normal(rng, shape, jnp.float32) * width * level
    return jnp.minimum(jnp.maximum(values, -most), most).astype(kind)


def setup_inputs(seed: int = 0) -> dict:
    streams_of = jax.random.split(jax.random.key(seed), 20)
    tokens = bell_draw(streams_of[0], (SEQUENCE_TOTAL, D), 1.0, 6.0, ((0, 16),))
    norm_gain_attn = jnp.clip(1.0 + 0.18 * jax.random.normal(streams_of[1], (D,), jnp.float32), 0.1, 1.9)
    w_query = bell_draw(streams_of[2], (D, HEAD_TOTAL * HEAD_DIM), D ** -0.5, 0.125, ((0, 16), (1, 2)))
    w_key = bell_draw(streams_of[3], (D, KV_HEADS * HEAD_DIM), D ** -0.5, 0.125, ((0, 16), (1, 2)))
    w_value = bell_draw(streams_of[4], (D, KV_HEADS * HEAD_DIM), D ** -0.5, 0.125, ((0, 16), (1, 2)))
    w_forget = bell_draw(streams_of[5], (D, HEAD_TOTAL), D ** -0.5, 0.125, ((1, 2),))
    forget_bias = jnp.clip(-1.0 + 4.0 * jax.random.uniform(streams_of[6], (HEAD_TOTAL,), jnp.float32) ** block_levels(streams_of[6], (HEAD_TOTAL,), ((0, 2),), -0.2, 0.2), -1.0, 3.0)
    cache_keys = draw_cache_keys(jax.random.fold_in(streams_of[19], 71), 0)
    cache_values = bell_draw(streams_of[8], (SEQUENCE_TOTAL, KV_HEADS * HEAD_DIM, LENGTH_LIMIT), 1.0, 6.0, ((0, 16), (1, 2)))
    cache_logcum = draw_cache_logcum(jax.random.fold_in(streams_of[19], 71), 0)
    lengths = draw_lengths(jax.random.fold_in(streams_of[19], 71), 0)
    w_out = bell_draw(streams_of[11], (HEAD_TOTAL * HEAD_DIM, D), (HEAD_TOTAL * HEAD_DIM) ** -0.5, 0.125, ((0, 2),))
    norm_gain_mix = jnp.clip(1.0 + 0.18 * jax.random.normal(streams_of[12], (D,), jnp.float32), 0.1, 1.9)
    norm_gain_ffn = jnp.clip(1.0 + 0.18 * jax.random.normal(streams_of[13], (D,), jnp.float32), 0.1, 1.9)
    expert_gate = bell_draw(streams_of[14], (D, EXPERTS * FF), D ** -0.5, 0.125, ((1, 32),))
    expert_up = bell_draw(streams_of[15], (D, EXPERTS * FF), D ** -0.5, 0.125, ((1, 32),))
    expert_down = bell_draw(streams_of[16], (EXPERTS * FF, D), FF ** -0.5, 0.09375, ((0, 32),))
    routes_keys = jax.random.split(jax.random.fold_in(streams_of[17], 1), SEQUENCE_TOTAL // B_DEV)
    routes_turns = jax.random.permutation(jax.random.fold_in(streams_of[17], 3), SEQUENCE_TOTAL // B_DEV)
    routes = jax.vmap(lambda own, number: assign_block(jax.random.fold_in(streams_of[17], 2), own, number, B_DEV, EXPERTS, TOP, CAP, 2))(routes_keys, routes_turns).reshape((SEQUENCE_TOTAL, TOP))
    route_weights = jnp.clip(jnp.exp(math.log(1.0) - 1.609438 * jax.random.uniform(streams_of[18], (SEQUENCE_TOTAL, TOP), jnp.float32) ** block_levels(streams_of[18], (SEQUENCE_TOTAL, TOP), ((0, 16),), -0.2, 0.2)), 0.2, 1.0)
    return dict(tokens=tokens, norm_gain_attn=norm_gain_attn, w_query=w_query, w_key=w_key, w_value=w_value, w_forget=w_forget, forget_bias=forget_bias, cache_keys=cache_keys, cache_values=cache_values, cache_logcum=cache_logcum, lengths=lengths, w_out=w_out, norm_gain_mix=norm_gain_mix, norm_gain_ffn=norm_gain_ffn, expert_gate=expert_gate, expert_up=expert_up, expert_down=expert_down, routes=routes, route_weights=route_weights)


EPSILON = 1e-06
MASKED = -1e+30

def rms_scaled(field, gain_vector):
    return field * lax.rsqrt(lax.optimization_barrier(jnp.mean(field * field, axis=-1, keepdims=True)) + EPSILON) * gain_vector

def attend(query, new_key, new_value, log_gate, key_cache, value_cache, logcum, seq_lengths):
    count = query.shape[0]
    scale = HEAD_DIM ** (-0.5)
    group = HEAD_TOTAL // KV_HEADS
    query_heads = query.astype(jnp.float32).reshape(count, KV_HEADS, group, HEAD_DIM)
    key_heads = key_cache.astype(jnp.float32).reshape(count, KV_HEADS, HEAD_DIM, LENGTH_LIMIT)
    value_heads = value_cache.astype(jnp.float32).reshape(count, KV_HEADS, HEAD_DIM, LENGTH_LIMIT)
    scores = jnp.einsum('bkgd,bkdl->bkgl', query_heads, key_heads).reshape(count, HEAD_TOTAL, LENGTH_LIMIT) * scale
    own_key = new_key.astype(jnp.float32).reshape(count, KV_HEADS, 1, HEAD_DIM)
    own_score = lax.optimization_barrier(jnp.sum(query_heads * own_key, axis=-1)).reshape(count, HEAD_TOTAL) * scale
    index = jnp.broadcast_to((seq_lengths - 1).astype(jnp.int32)[:, None, None], (count, HEAD_TOTAL, 1))
    last_cum = jnp.take_along_axis(logcum, index, axis=2)[:, :, 0]
    shift = (last_cum + log_gate)[:, :, None] - logcum
    places = jnp.arange(LENGTH_LIMIT, dtype=jnp.int32)
    valid = (places[None, :] < seq_lengths[:, None])[:, None, :]
    past = jnp.where(valid, scores + shift, MASKED)
    peak = jnp.maximum(lax.optimization_barrier(jnp.max(past, axis=-1)), own_score)
    past_exp = jnp.exp(past - peak[:, :, None])
    own_exp = jnp.exp(own_score - peak)
    total = lax.optimization_barrier(jnp.sum(past_exp, axis=-1)) + own_exp
    past_weight = lax.optimization_barrier((past_exp / total[:, :, None]).astype(jnp.bfloat16)).astype(jnp.float32)
    own_weight = lax.optimization_barrier((own_exp / total).astype(jnp.bfloat16)).astype(jnp.float32)
    past_weight = past_weight.reshape(count, KV_HEADS, group, LENGTH_LIMIT)
    mixed = jnp.einsum('bkgl,bkdl->bkgd', past_weight, value_heads)
    own_value = new_value.astype(jnp.float32).reshape(count, KV_HEADS, 1, HEAD_DIM)
    mixed = mixed + own_weight.reshape(count, KV_HEADS, group)[:, :, :, None] * own_value
    return mixed.astype(jnp.bfloat16).reshape(count, HEAD_TOTAL * HEAD_DIM)

def reference(tokens, norm_gain_attn, w_query, w_key, w_value, w_forget, forget_bias, cache_keys, cache_values, cache_logcum, lengths, w_out, norm_gain_mix, norm_gain_ffn, expert_gate, expert_up, expert_down, routes, route_weights):
    residual = tokens.astype(jnp.float32)
    normed = rms_scaled(residual, norm_gain_attn).astype(jnp.bfloat16)
    query = jnp.dot(normed, w_query, preferred_element_type=jnp.float32).astype(jnp.bfloat16)
    new_keys = jnp.dot(normed, w_key, preferred_element_type=jnp.float32).astype(jnp.bfloat16)
    new_values = jnp.dot(normed, w_value, preferred_element_type=jnp.float32).astype(jnp.bfloat16)
    new_log_gate = jax.nn.log_sigmoid(jnp.dot(normed, w_forget, preferred_element_type=jnp.float32) + forget_bias)
    groups = SEQUENCE_TOTAL // B_DEV

    def by_group(array):
        return array.reshape((groups, B_DEV) + array.shape[1:])

    def one_group(items):
        return attend(*items)
    heads_out = lax.map(one_group, (by_group(query), by_group(new_keys), by_group(new_values), by_group(new_log_gate), by_group(cache_keys), by_group(cache_values), by_group(cache_logcum), by_group(lengths)))
    heads_out = heads_out.reshape(SEQUENCE_TOTAL, HEAD_TOTAL * HEAD_DIM)
    head_width = HEAD_TOTAL * HEAD_DIM // N_TP
    grouped_out = heads_out.astype(jnp.float32).reshape(SEQUENCE_TOTAL, N_TP, head_width)
    grouped_w = w_out.astype(jnp.float32).reshape(N_TP, head_width, D)
    partials = jnp.einsum('stc,tcd->tsd', grouped_out, grouped_w)
    partials = lax.optimization_barrier(partials.astype(jnp.bfloat16)).astype(jnp.float32)
    mix = lax.optimization_barrier(jnp.sum(partials, axis=0))
    mixed_res = residual + rms_scaled(mix, norm_gain_mix)
    ffn_in = rms_scaled(mixed_res, norm_gain_ffn).astype(jnp.bfloat16)

    def expert_step(carry, expert_index):
        start = expert_index * FF
        gate_part = jnp.dot(ffn_in, lax.dynamic_slice_in_dim(expert_gate, start, FF, 1), preferred_element_type=jnp.float32)
        up_part = jnp.dot(ffn_in, lax.dynamic_slice_in_dim(expert_up, start, FF, 1), preferred_element_type=jnp.float32)
        hidden = (jax.nn.silu(gate_part) * up_part).astype(jnp.bfloat16)
        expert_out = jnp.dot(hidden, lax.dynamic_slice_in_dim(expert_down, start, FF, 0), preferred_element_type=jnp.float32)
        weight = lax.optimization_barrier(jnp.sum(jnp.where(routes == expert_index, route_weights, 0.0), axis=1))
        return (carry + weight[:, None] * expert_out, None)
    routed, _ = lax.scan(expert_step, jnp.zeros((SEQUENCE_TOTAL, D), jnp.float32), jnp.arange(EXPERTS, dtype=jnp.int32))
    layer_out = (mixed_res + routed).astype(jnp.bfloat16)
    return (layer_out, new_keys, new_values, new_log_gate)
```

```python
import functools

import jax
import jax.numpy as jnp
from jax import lax
from jax.experimental import pallas as pl
from jax.experimental.pallas import tpu as pltpu
from jax.sharding import PartitionSpec as P

HEAD_TOTAL = 32
KV_HEADS = 4
HEAD_DIM = 64
SPAN = 4
TOP = 2


EPSILON = 1e-06
MASKED = -1e30


def rms_scaled(field, gain_vector):
    return (
        field * lax.rsqrt(jnp.mean(field * field, axis=-1, keepdims=True) + EPSILON) * gain_vector
    )


VMEM = pltpu.VMEM
MESH = pl.DeviceIdType.MESH
BF16 = jnp.bfloat16
F32 = jnp.float32


def bit_count(devices):
    return devices.bit_length() - 1


def reversed_bits(place, bits):
    return sum(((place >> b) & 1) << (bits - 1 - b) for b in range(bits))


def flipped(me, mask, bits):
    other = me
    for b in range(bits):
        if (mask >> b) & 1:
            other = other + (1 - 2 * ((me // (1 << b)) % 2)) * (1 << b)
    return other


def greet(partners):
    barrier = pltpu.get_barrier_semaphore()
    for partner in partners:
        pl.semaphore_signal(barrier, inc=1, device_id=partner, device_id_type=MESH)
    pl.semaphore_wait(barrier, len(partners))


def remote(src, dst, send_sem, recv_sem, partner):
    return pltpu.make_async_remote_copy(
        src_ref=src,
        dst_ref=dst,
        send_sem=send_sem,
        recv_sem=recv_sem,
        device_id=partner,
        device_id_type=MESH,
    )


def add_into(acc, got, low, high, shift, cols):
    acc[low:high, :, cols] = (
        acc[low:high, :, cols].astype(F32) + got[low + shift : high + shift, :, cols].astype(F32)
    ).astype(BF16)


def copy_of(src, dst, sem):
    return pltpu.make_async_copy(src_ref=src, dst_ref=dst, sem=sem)


def normalized(field):
    return field * lax.rsqrt(jnp.mean(field * field, axis=-1, keepdims=True) + EPSILON)


def front_kernel(
    zs,
    chunk,
    tok_hbm,
    gain_hbm,
    wq_hbm,
    wk_hbm,
    wv_hbm,
    wf_hbm,
    bias_hbm,
    kc_hbm,
    vc_hbm,
    cum_hbm,
    len_hbm,
    wo_hbm,
    gmix_hbm,
    gffn_hbm,
    nk_ref,
    nv_ref,
    gate_ref,
    res_ref,
    ffn_ref,
    tok,
    gattn,
    gmix,
    gffn,
    weights,
    wf,
    bias,
    kc,
    vc,
    cum,
    lens,
    wo,
    normed,
    xs,
    own,
    acc,
    got,
    qs,
    kn,
    vn,
    scores,
    probs,
    own_exp,
    inverse,
    outs,
    heads,
    part,
    theirs,
    local,
    xsend,
    xrecv,
    csend,
    crecv,
    fsend,
    frecv,
    tsend,
    trecv,
    zsend,
    zrecv,
    ysend,
    yrecv,
):
    me, tp = lax.axis_index("ep"), lax.axis_index("tp")
    place = me % SPAN
    z = me // SPAN
    core_peer = (me + 1 - 2 * (me % 2), tp)
    x_peer = (me + 2 - 4 * ((me // 2) % 2), tp)
    y_peer = (me, 1 - tp)

    def z_peer(d):
        return (((z + d + zs) % zs) * SPAN + place, tp)

    rows, width = tok.shape
    depth = wq_hbm.shape[0]
    query_cols = wq_hbm.shape[1]
    key_cols = wk_hbm.shape[1]
    slab = SPAN * depth
    total = weights.shape[1]
    chunks = total // chunk
    heads_here = query_cols // HEAD_DIM
    mine = pl.ds(pl.multiple_of(place * depth, depth), depth)
    x_place = place + 2 - 4 * ((me // 2) % 2)
    xs_rows = pl.ds(pl.multiple_of(x_place * depth, depth), depth)

    first = [
        copy_of(tok_hbm, tok, local.at[0]),
        copy_of(gain_hbm, gattn, local.at[1]),
        copy_of(wq_hbm, weights.at[mine, 0:query_cols], local.at[2]),
        copy_of(wk_hbm, weights.at[mine, query_cols : query_cols + key_cols], local.at[3]),
        copy_of(wv_hbm, weights.at[mine, query_cols + key_cols : total], local.at[4]),
        copy_of(wf_hbm, wf, local.at[5]),
        copy_of(bias_hbm, bias, local.at[6]),
        copy_of(len_hbm, lens, local.at[7]),
        copy_of(gmix_hbm, gmix, local.at[8]),
        copy_of(gffn_hbm, gffn, local.at[9]),
    ]
    later = [
        copy_of(kc_hbm, kc, local.at[10]),
        copy_of(vc_hbm, vc, local.at[11]),
        copy_of(cum_hbm, cum, local.at[12]),
        copy_of(wo_hbm, wo, local.at[13]),
    ]
    for move in first:
        move.start()
    barrier = pltpu.get_barrier_semaphore()
    partners = [core_peer, x_peer, y_peer] + [z_peer(d) for d in range(1, zs)]
    for partner in partners:
        pl.semaphore_signal(barrier, inc=1, device_id=partner, device_id_type=MESH)
    first[0].wait()
    first[1].wait()
    normed[...] = (normalized(tok[...].astype(F32)) * gattn[...]).astype(BF16)
    xs[0:rows, :] = normed[:, pl.ds(pl.multiple_of(z * slab, slab), slab)]
    for move in first[2:5]:
        move.wait()
    pl.semaphore_wait(barrier, len(partners))

    order = [chunks - 1] + list(range(chunks - 1))
    across, direct, forward, slabs, sums = {}, {}, {}, {}, {}
    for k in order:
        cols = pl.ds(k * chunk, chunk)
        view = weights.at[mine, cols]
        across[k] = remote(view, view, xsend.at[k], xrecv.at[k], x_peer)
        across[k].start()
        if k == order[0]:
            for d in range(1, zs):
                peer = z_peer(d)
                there = pl.ds(pl.multiple_of((peer[0] // SPAN) * slab, slab), slab)
                slabs[d] = remote(
                    normed.at[:, there],
                    xs.at[d * rows : (d + 1) * rows],
                    tsend.at[d],
                    trecv.at[d],
                    peer,
                )
                slabs[d].start()
    view = weights.at[mine]
    direct = remote(view, view, csend.at[0], crecv.at[0], core_peer)
    direct.start()
    for move in later:
        move.start()

    for move in first[5:7]:
        move.wait()
    logits = lax.dot_general(
        wf[...], normed[...], (((1,), (1,)), ((), ())), preferred_element_type=F32
    )
    row_of = lax.broadcasted_iota(jnp.int32, logits.shape, 0)
    for h in range(heads_here):
        logits = logits + jnp.where(row_of == h, bias[h], 0.0)
    gate_ref[...] = jnp.minimum(logits, 0.0) - jnp.log1p(jnp.exp(-jnp.abs(logits)))

    for d in range(1, zs):
        slabs[d].wait_recv()
    direct.wait_recv()
    for k in order:
        cols = pl.ds(k * chunk, chunk)
        across[k].wait_recv()
        view = weights.at[xs_rows, cols]
        forward[k] = remote(view, view, fsend.at[k], frecv.at[k], core_peer)
        forward[k].start()
        forward[k].wait_recv()
        product = jnp.dot(xs[...], weights[:, cols], preferred_element_type=F32)
        own[k] = product[0:rows]
        acc[k] = product[rows:].astype(BF16)
        for d in range(1, zs):
            sums[k, d] = remote(
                acc.at[k, (d - 1) * rows : d * rows],
                got.at[k, (d - 1) * rows : d * rows],
                zsend.at[k, d],
                zrecv.at[k, d],
                z_peer(-d),
            )
            sums[k, d].start()

    lane = lax.broadcasted_iota(jnp.int32, (rows, 2 * HEAD_DIM), 1)
    low = lane < HEAD_DIM
    for k in order:
        value = own[k]
        for d in range(1, zs):
            sums[k, d].wait_recv()
            value = value + got[k, (d - 1) * rows : d * rows, :].astype(F32)
        value = value.astype(BF16)
        if k == order[0]:
            nk_ref[...] = value[:, 0:key_cols]
            nv_ref[...] = value[:, key_cols:]
            kn[...] = value[:, 0:key_cols].astype(F32)
            vn[...] = value[:, key_cols:].astype(F32)
            continue
        value = value.astype(F32) * (HEAD_DIM**-0.5)
        for j in range(chunk // (2 * HEAD_DIM)):
            block = value[:, j * 2 * HEAD_DIM : (j + 1) * 2 * HEAD_DIM]
            rolled = pltpu.roll(block, HEAD_DIM, 1)
            head = (k * chunk) // HEAD_DIM + 2 * j
            if head < heads_here // 2:
                pair = (jnp.where(low, block, 0.0), jnp.where(low, rolled, 0.0))
            else:
                pair = (jnp.where(low, 0.0, rolled), jnp.where(low, 0.0, block))
            qs[pl.ds(head, rows, stride=heads_here), :] = pair[0]
            qs[pl.ds(head + 1, rows, stride=heads_here), :] = pair[1]

    for move in later:
        move.wait()
    first[7].wait()
    unroll = 4
    groups = rows // unroll
    span_len = cum.shape[2]
    places = lax.broadcasted_iota(jnp.int32, (heads_here, span_len), 1)
    lane_b = lax.broadcasted_iota(jnp.int32, gate_ref.shape, 1)

    def strip(b):
        return pl.ds(pl.multiple_of(b * heads_here, heads_here), heads_here)

    def score(g):
        for u in range(unroll):
            b = g * unroll + u
            scores[strip(b), :] = jnp.dot(
                qs[strip(b), :].astype(BF16), kc[b], preferred_element_type=F32
            )

    def soften(g):
        for u in range(unroll):
            b = g * unroll + u
            length = lens[b]
            logcum = cum[b]
            gate = jnp.sum(jnp.where(lane_b == b, gate_ref[...], 0.0), axis=1, keepdims=True)
            last = jnp.sum(jnp.where(places == length - 1, logcum, 0.0), axis=1, keepdims=True)
            mine_score = jnp.sum(qs[strip(b), :] * kn[pl.ds(b, 1), :], axis=1, keepdims=True)
            past = scores[strip(b), :] + ((last + gate) - logcum)
            past = jnp.where(places < length, past, MASKED)
            peak = jnp.maximum(jnp.max(past, axis=1, keepdims=True), mine_score)
            raised = jnp.exp(past - peak)
            mine_exp = jnp.exp(mine_score - peak)
            probs[strip(b), :] = raised.astype(BF16)
            sum_all = jnp.sum(raised, axis=1, keepdims=True) + mine_exp
            own_exp[strip(b), :] = jnp.broadcast_to(mine_exp, (heads_here, key_cols))
            inverse[strip(b), :] = jnp.broadcast_to(1.0 / sum_all, (heads_here, key_cols))

    def weigh(g):
        for u in range(unroll):
            b = g * unroll + u
            mixed = lax.dot_general(
                probs[strip(b), :],
                vc[b],
                (((1,), (1,)), ((), ())),
                preferred_element_type=F32,
            )
            mixed = mixed + own_exp[strip(b), :] * vn[pl.ds(b, 1), :]
            outs[strip(b), :] = mixed * inverse[strip(b), :]

    def turn(g, carry):
        weigh(g - 2)
        soften(g - 1)
        score(g)
        return carry

    score(0)
    soften(0)
    score(1)
    lax.fori_loop(2, groups, turn, 0)
    weigh(groups - 2)
    soften(groups - 1)
    weigh(groups - 1)

    for m in range(heads_here // 2):
        a = outs[pl.ds(2 * m, rows, stride=heads_here), :]
        b = outs[pl.ds(2 * m + 1, rows, stride=heads_here), :]
        if 2 * m < heads_here // 2:
            b = pltpu.roll(b, HEAD_DIM, 1)
        else:
            a = pltpu.roll(a, HEAD_DIM, 1)
        heads[:, m * 2 * HEAD_DIM : (m + 1) * 2 * HEAD_DIM] = jnp.where(low, a, b).astype(BF16)

    piece = 2 * chunk
    swaps = {}
    for n in range(width // piece):
        cols = pl.ds(n * piece, piece)
        part[:, cols] = jnp.dot(
            heads[...], wo[:, cols], preferred_element_type=F32
        ).astype(BF16)
        swaps[n] = remote(
            part.at[:, cols], theirs.at[:, cols], ysend.at[n], yrecv.at[n], y_peer
        )
        swaps[n].start()
    for move in first[8:10]:
        move.wait()
    for n in swaps:
        swaps[n].wait_recv()
    mix = part[...].astype(F32) + theirs[...].astype(F32)
    mixed_res = tok[...].astype(F32) + normalized(mix) * gmix[...]
    res_ref[...] = mixed_res
    ffn_ref[...] = (normalized(mixed_res) * gffn[...]).astype(BF16)

    direct.wait_send()
    for k in order:
        across[k].wait_send()
        forward[k].wait_send()
    for d in slabs:
        slabs[d].wait_send()
    for key in sums:
        sums[key].wait_send()
    for n in swaps:
        swaps[n].wait_send()


def dispatch_kernel(
    devices,
    chunks,
    rows_ref,
    wts_ref,
    all_ref,
    wall_ref,
    tsend,
    trecv,
    send,
    recv,
    wsend,
    wrecv,
):
    bits = bit_count(devices)
    me, tp = lax.axis_index("ep"), lax.axis_index("tp")
    other_tp = (me, 1 - tp)
    partners = [(flipped(me, 1 << b, bits), tp) for b in range(bits)]
    greet(partners + [other_tp])
    wall_ref[0] = wts_ref[...]
    all_ref[0] = rows_ref[...]
    width = all_ref.shape[2] // chunks
    copies = {}
    shared = chunks - 2
    half = 1 << (bits - 1)

    def columns(c):
        piece = chunks - 2 + tp if c == shared else c
        return pl.ds(pl.multiple_of(piece * width, width), width)

    def exchange(step, c, cols=None):
        n = 1 << step
        partner = partners[bits - 1 - step]
        if c < chunks:
            cols = columns(c) if cols is None else cols
            move = remote(
                all_ref.at[0:n, :, cols],
                all_ref.at[n : 2 * n, :, cols],
                send.at[step, c],
                recv.at[step, c],
                partner,
            )
        else:
            move = remote(
                wall_ref.at[0:n], wall_ref.at[n : 2 * n], wsend.at[step], wrecv.at[step], partner
            )
        copies[step, c] = move
        move.start()

    order = [shared] + list(range(shared)) + [chunks]
    for step in range(bits - 1):
        for c in order:
            if step:
                copies[step - 1, c].wait_recv()
            exchange(step, c)
    copies[bits - 2, shared].wait_recv()
    across = remote(
        all_ref.at[1:half, :, columns(shared)],
        all_ref.at[1:half, :, columns(shared)],
        tsend.at[1],
        trecv.at[1],
        other_tp,
    )
    across.start()
    exchange(bits - 1, shared)
    for c in order[1:]:
        copies[bits - 2, c].wait_recv()
        exchange(bits - 1, c)
    across.wait_recv()
    theirs_cols = pl.ds(pl.multiple_of((chunks - 1 - tp) * width, width), width)
    exchange(bits - 1, chunks - 1, theirs_cols)
    for c in order + [chunks - 1]:
        copies[bits - 1, c].wait_recv()
    across.wait_send()
    for key in copies:
        copies[key].wait_send()


def combine_kernel(devices, chunk, acc_in, out_ref, acc, got0, got1, got, send, recv):
    bits = bit_count(devices)
    me, tp = lax.axis_index("ep"), lax.axis_index("tp")
    partners = [(flipped(me, 1 << b, bits), tp) for b in range(bits)]
    other_tp = (me, 1 - tp)
    greet(partners + [other_tp])
    half = devices // 2
    share = acc.shape[2]
    chunks = share // chunk
    copies = {}

    def ds(side, c):
        return pl.ds(pl.multiple_of(side * share + c * chunk, 128), chunk)

    for side in range(2):
        for c in range(chunks):
            where = ds(1 - tp, c) if side == 0 else ds(tp, c)
            copies[0, side, c] = remote(
                acc_in.at[half:devices, :, where],
                got0.at[side, :, :, pl.ds(c * chunk, chunk)],
                send.at[side, c],
                recv.at[side, c],
                partners[0],
            )
            copies[0, side, c].start()
    outgoing = got1.at[0]
    incoming = got1.at[1]
    for c in range(chunks):
        cols = slice(c * chunk, (c + 1) * chunk)
        copies[0, 0, c].wait_recv()
        outgoing[:, :, cols] = (
            acc_in[0:half, :, ds(1 - tp, c)].astype(F32) + got0[0, :, :, cols].astype(F32)
        ).astype(BF16)
        copies[1, 0, c] = remote(
            outgoing.at[:, :, pl.ds(c * chunk, chunk)],
            incoming.at[:, :, pl.ds(c * chunk, chunk)],
            send.at[2, c],
            recv.at[2, c],
            other_tp,
        )
        copies[1, 0, c].start()
    for c in range(chunks):
        cols = slice(c * chunk, (c + 1) * chunk)
        copies[0, 1, c].wait_recv()
        acc[:, :, cols] = (
            acc_in[0:half, :, ds(tp, c)].astype(F32) + got0[1, :, :, cols].astype(F32)
        ).astype(BF16)

    def exchange(step, c):
        n = half >> step
        copies[step + 1, 0, c] = remote(
            acc.at[n : 2 * n, :, pl.ds(c * chunk, chunk)],
            got.at[n : 2 * n, :, pl.ds(c * chunk, chunk)],
            send.at[step + 2, c],
            recv.at[step + 2, c],
            partners[step],
        )
        copies[step + 1, 0, c].start()

    for step in range(bits):
        n = half >> step
        source = incoming if step == 0 else got
        shift = 0 if step == 0 else n
        for c in range(chunks):
            copies[step + 1, 0, c].wait_recv()
            cols = slice(c * chunk, (c + 1) * chunk)
            if step + 1 < bits:
                add_into(acc, source, n // 2, n, shift, cols)
                exchange(step + 1, c)
                add_into(acc, source, 0, n // 2, shift, cols)
            else:
                out_ref[:, cols] = acc[0, :, cols].astype(F32) + source[
                    shift, :, cols
                ].astype(F32)
    for key in copies:
        copies[key].wait_send()


def communicate(kernel, out_shape, scratch, number, *operands, places=VMEM):
    whole = pl.BlockSpec(memory_space=VMEM)
    many = isinstance(out_shape, tuple)
    return pl.pallas_call(
        kernel,
        out_shape=out_shape,
        in_specs=[pl.BlockSpec(memory_space=places)] * len(operands),
        out_specs=(whole,) * len(out_shape) if many else whole,
        scratch_shapes=scratch,
        compiler_params=pltpu.CompilerParams(
            collective_id=number, has_side_effects=True, vmem_limit_bytes=50 * 1024 * 1024
        ),
    )(*operands)


def body(
    tokens,
    norm_gain_attn,
    w_query,
    w_key,
    w_value,
    w_forget,
    forget_bias,
    cache_keys,
    cache_values,
    cache_logcum,
    lengths,
    w_out,
    norm_gain_mix,
    norm_gain_ffn,
    expert_gate,
    expert_up,
    expert_down,
    routes,
    route_weights,
):
    row_count = tokens.shape[0]
    model_width = tokens.shape[1]
    query_cols = w_query.shape[1]
    key_cols = w_key.shape[1]
    residual = tokens.astype(jnp.float32)
    normed = rms_scaled(residual, norm_gain_attn).astype(jnp.bfloat16)
    devices = lax.axis_size("ep")
    expert_count = devices // SPAN
    slot_count = max(2, min(row_count, 2 * row_count * TOP // expert_count))
    depth = w_query.shape[0]
    joint_cols = query_cols + 2 * key_cols
    chunk = 256
    dense = (
        slot_count == row_count
        and lax.axis_size("tp") == 2
        and devices & (devices - 1) == 0
        and depth % 128 == 0
        and joint_cols % chunk == 0
        and devices % SPAN == 0
        and key_cols == 2 * HEAD_DIM
        and 2 * key_cols == chunk
        and row_count % 8 == 0
        and model_width % (2 * chunk) == 0
    )
    if dense:
        bits = bit_count(devices)
        dma = pltpu.SemaphoreType.DMA
        zs = devices // SPAN
        chunks = joint_cols // chunk
        heads_here = query_cols // HEAD_DIM
        strips = row_count * heads_here
        smem = pltpu.SMEM
        pieces = model_width // (2 * chunk)
        new_keys, new_values, gate_rows, mixed_res, ffn_in = communicate(
            functools.partial(front_kernel, zs, chunk),
            (
                jax.ShapeDtypeStruct((row_count, key_cols), BF16),
                jax.ShapeDtypeStruct((row_count, key_cols), BF16),
                jax.ShapeDtypeStruct((heads_here, row_count), F32),
                jax.ShapeDtypeStruct((row_count, model_width), F32),
                jax.ShapeDtypeStruct((row_count, model_width), BF16),
            ),
            [
                VMEM((row_count, model_width), BF16),
                VMEM((1, model_width), F32),
                VMEM((1, model_width), F32),
                VMEM((1, model_width), F32),
                VMEM((SPAN * depth, joint_cols), BF16),
                VMEM((heads_here, model_width), BF16),
                smem((heads_here,), F32),
                VMEM(cache_keys.shape, BF16),
                VMEM(cache_values.shape, BF16),
                VMEM(cache_logcum.shape, F32),
                smem((row_count,), jnp.int32),
                VMEM(w_out.shape, BF16),
                VMEM((row_count, model_width), BF16),
                VMEM((zs * row_count, SPAN * depth), BF16),
                VMEM((chunks, row_count, chunk), F32),
                VMEM((chunks, (zs - 1) * row_count, chunk), BF16),
                VMEM((chunks, (zs - 1) * row_count, chunk), BF16),
                VMEM((strips, key_cols), F32),
                VMEM((row_count, key_cols), F32),
                VMEM((row_count, key_cols), F32),
                VMEM((strips, cache_keys.shape[2]), F32),
                VMEM((strips, cache_keys.shape[2]), BF16),
                VMEM((strips, key_cols), F32),
                VMEM((strips, key_cols), F32),
                VMEM((strips, key_cols), F32),
                VMEM((row_count, query_cols), BF16),
                VMEM((row_count, model_width), BF16),
                VMEM((row_count, model_width), BF16),
                dma((14,)),
                dma((chunks,)),
                dma((chunks,)),
                dma((1,)),
                dma((1,)),
                dma((chunks,)),
                dma((chunks,)),
                dma((zs,)),
                dma((zs,)),
                dma((chunks, zs)),
                dma((chunks, zs)),
                dma((pieces,)),
                dma((pieces,)),
            ],
            1,
            tokens,
            norm_gain_attn.reshape(1, -1),
            w_query,
            w_key,
            w_value,
            w_forget.T,
            forget_bias,
            cache_keys,
            cache_values,
            cache_logcum,
            lengths,
            w_out,
            norm_gain_mix.reshape(1, -1),
            norm_gain_ffn.reshape(1, -1),
            places=pl.ANY,
        )
        new_log_gate = gate_rows.T
        chosen = (routes[:, :, None] == jnp.arange(expert_count, dtype=jnp.int32)).astype(F32)
        weights = jnp.sum(chosen * route_weights[:, :, None], axis=1)
        upper = weights.astype(BF16)
        lower = (weights - upper.astype(F32)).astype(BF16)
        lanes = 128
        weights = jnp.concatenate((upper, lower), axis=1)
        weights = jnp.pad(weights, ((0, 0), (0, lanes - weights.shape[1])))
        rows_all, weights_all = communicate(
            functools.partial(dispatch_kernel, devices, pieces),
            (
                jax.ShapeDtypeStruct((devices, row_count, model_width), BF16),
                jax.ShapeDtypeStruct((devices, row_count, lanes), BF16),
            ),
            [
                dma((2,)),
                dma((2,)),
                dma((bits, pieces)),
                dma((bits, pieces)),
                dma((bits,)),
                dma((bits,)),
            ],
            2,
            ffn_in,
            weights,
        )
        flat_rows = rows_all.reshape(devices * row_count, model_width)
        gate_part = jnp.dot(flat_rows, expert_gate, preferred_element_type=F32)
        up_part = jnp.dot(flat_rows, expert_up, preferred_element_type=F32)
        hidden = (jax.nn.silu(gate_part) * up_part).astype(BF16)
        expert_part = jnp.dot(hidden, expert_down, preferred_element_type=F32)
        mine = lax.axis_index("ep") // SPAN
        lane = jnp.arange(lanes, dtype=jnp.int32)
        picked = ((lane == mine) | (lane == mine + expert_count)).astype(F32)
        own_weight = jnp.sum(weights_all.astype(F32) * picked, axis=2).reshape(-1, 1)
        share = model_width // 2
        part = (expert_part * own_weight).astype(BF16)
        half = devices // 2
        routed = communicate(
            functools.partial(combine_kernel, devices, chunk),
            jax.ShapeDtypeStruct((row_count, share), F32),
            [
                VMEM((half, row_count, share), BF16),
                VMEM((2, half, row_count, share), BF16),
                VMEM((2, half, row_count, share), BF16),
                VMEM((half, row_count, share), BF16),
                dma((bits + 2, share // chunk)),
                dma((bits + 2, share // chunk)),
            ],
            3,
            part.reshape(devices, row_count, model_width),
        )
        residual_cols = lax.dynamic_slice_in_dim(
            mixed_res, lax.axis_index("tp") * share, share, 1
        )
        layer_out = (residual_cols + routed).astype(BF16)
        return (layer_out, new_keys, new_values, new_log_gate)
    joined = jnp.concatenate(
        (
            lax.all_gather(w_query, "ep", axis=0, tiled=True),
            lax.all_gather(w_key, "ep", axis=0, tiled=True),
            lax.all_gather(w_value, "ep", axis=0, tiled=True),
        ),
        axis=1,
    )
    projected = jnp.dot(normed, joined, preferred_element_type=jnp.float32)
    query = projected[:, :query_cols].astype(jnp.bfloat16)
    new_keys = projected[:, query_cols : query_cols + key_cols].astype(jnp.bfloat16)
    new_values = projected[:, query_cols + key_cols :].astype(jnp.bfloat16)
    new_log_gate = jax.nn.log_sigmoid(
        jnp.dot(normed, w_forget, preferred_element_type=jnp.float32) + forget_bias
    )
    local_heads = query_cols // HEAD_DIM
    local_kv = key_cols // HEAD_DIM
    group = HEAD_TOTAL // KV_HEADS
    span_len = cache_keys.shape[2]
    scale = HEAD_DIM ** (-0.5)
    query_heads = query.reshape(row_count, local_kv, group, HEAD_DIM)
    key_heads = cache_keys.reshape(row_count, local_kv, HEAD_DIM, span_len)
    value_heads = cache_values.reshape(row_count, local_kv, HEAD_DIM, span_len)
    scores = jnp.einsum(
        "bkgd,bkdl->bkgl", query_heads, key_heads, preferred_element_type=jnp.float32
    )
    scores = scores.reshape(row_count, local_heads, span_len) * scale
    own_key = new_keys.astype(jnp.float32).reshape(row_count, local_kv, 1, HEAD_DIM)
    own_score = (
        jnp.sum(query_heads.astype(jnp.float32) * own_key, axis=-1).reshape(row_count, local_heads)
        * scale
    )
    places = jnp.arange(span_len, dtype=jnp.int32)
    at_last = (places[None, :] == (lengths - 1)[:, None]).astype(jnp.float32)
    last_cum = jnp.sum(cache_logcum * at_last[:, None, :], axis=2)
    shift = (last_cum + new_log_gate)[:, :, None] - cache_logcum
    valid = (places[None, :] < lengths[:, None])[:, None, :]
    past = jnp.where(valid, scores + shift, MASKED)
    peak = jnp.maximum(jnp.max(past, axis=-1), own_score)
    past_exp = jnp.exp(past - peak[:, :, None])
    own_exp = jnp.exp(own_score - peak)
    total = jnp.sum(past_exp, axis=-1) + own_exp
    past_weight = (
        (past_exp / total[:, :, None])
        .astype(jnp.bfloat16)
        .reshape(row_count, local_kv, group, span_len)
    )
    own_weight = (
        (own_exp / total)
        .astype(jnp.bfloat16)
        .astype(jnp.float32)
        .reshape(row_count, local_kv, group)
    )
    mixed = jnp.einsum(
        "bkgl,bkdl->bkgd", past_weight, value_heads, preferred_element_type=jnp.float32
    )
    own_value = new_values.astype(jnp.float32).reshape(row_count, local_kv, 1, HEAD_DIM)
    mixed = mixed + own_weight[:, :, :, None] * own_value
    heads_out = mixed.astype(jnp.bfloat16).reshape(row_count, query_cols)
    partial_mix = (
        jnp.dot(heads_out, w_out, preferred_element_type=jnp.float32)
        .astype(jnp.bfloat16)
        .astype(jnp.float32)
    )
    mix = lax.psum(partial_mix.astype(jnp.bfloat16), "tp").astype(jnp.float32)
    mixed_res = residual + rms_scaled(mix, norm_gain_mix)
    ffn_in = rms_scaled(mixed_res, norm_gain_ffn).astype(jnp.bfloat16)
    flat_routes = routes.reshape(-1)
    expert_hits = (
        flat_routes[:, None] == jnp.arange(expert_count, dtype=jnp.int32)[None, :]
    ).astype(jnp.int32)
    earlier = jnp.cumsum(expert_hits, axis=0) - expert_hits
    slot_index = jnp.sum(earlier * expert_hits, axis=1)
    in_slot = (slot_index[:, None] == jnp.arange(slot_count, dtype=jnp.int32)[None, :]).astype(
        jnp.float32
    )
    placing = expert_hits.astype(jnp.float32)[:, :, None] * in_slot[:, None, :]
    placing = placing.reshape(row_count, TOP, expert_count * slot_count)
    selector = jnp.sum(placing, axis=1).astype(jnp.bfloat16)
    weighing = jnp.sum(placing * route_weights[:, :, None], axis=1)
    packed = jnp.einsum("ra,rd->ad", selector, ffn_in, preferred_element_type=jnp.float32).astype(
        jnp.bfloat16
    )
    outgoing = jnp.broadcast_to(
        packed.reshape(expert_count, 1, slot_count, model_width),
        (expert_count, SPAN, slot_count, model_width),
    )
    outgoing = outgoing.reshape(expert_count * SPAN, slot_count, model_width)
    arrived = lax.all_to_all(outgoing, "ep", split_axis=0, concat_axis=0, tiled=True)
    sources, slots, width = arrived.shape
    flat_rows = arrived.reshape(sources * slots, width)
    gate_part = jnp.dot(flat_rows, expert_gate, preferred_element_type=jnp.float32)
    up_part = jnp.dot(flat_rows, expert_up, preferred_element_type=jnp.float32)
    hidden = (jax.nn.silu(gate_part) * up_part).astype(jnp.bfloat16)
    expert_part = jnp.dot(hidden, expert_down, preferred_element_type=jnp.float32)
    col_share = lax.psum_scatter(
        expert_part.astype(jnp.bfloat16), "tp", scatter_dimension=1, tiled=True
    ).astype(jnp.float32)
    returned = lax.all_to_all(
        col_share.reshape(sources, slots, -1).astype(jnp.bfloat16),
        "ep",
        split_axis=0,
        concat_axis=0,
        tiled=True,
    ).astype(jnp.float32)
    col_width = returned.shape[2]
    per_expert = jnp.sum(returned.reshape(expert_count, SPAN, slot_count, col_width), axis=1)
    per_expert = per_expert.reshape(expert_count * slot_count, col_width)
    routed = jnp.dot(
        weighing, per_expert, precision=lax.Precision.HIGHEST, preferred_element_type=jnp.float32
    )
    col_start = lax.axis_index("tp") * col_width
    residual_cols = lax.dynamic_slice_in_dim(mixed_res, col_start, col_width, 1)
    layer_out = (residual_cols + routed).astype(jnp.bfloat16)
    return (layer_out, new_keys, new_values, new_log_gate)


def solution(mesh):
    placed = (
        P("ep", None),
        P(),
        P("ep", "tp"),
        P("ep", "tp"),
        P("ep", "tp"),
        P(None, "tp"),
        P("tp"),
        P("ep", "tp", None),
        P("ep", "tp", None),
        P("ep", "tp", None),
        P("ep"),
        P("tp", None),
        P(),
        P(),
        P(None, ("ep", "tp")),
        P(None, ("ep", "tp")),
        P(("ep", "tp"), None),
        P("ep", None),
        P("ep", None),
    )
    return jax.shard_map(
        body,
        mesh=mesh,
        in_specs=placed,
        out_specs=(P("ep", "tp"), P("ep", "tp"), P("ep", "tp"), P("ep", "tp")),
        check_vma=False,
    )
```

```python
import functools

import jax
import jax.numpy as jnp
from jax import lax
from jax.experimental import pallas as pl
from jax.experimental.pallas import tpu as pltpu
from jax.sharding import PartitionSpec as P

HEAD_TOTAL = 32
KV_HEADS = 4
HEAD_DIM = 64
SPAN = 4
TOP = 2


EPSILON = 1e-06
MASKED = -1e30


def rms_scaled(field, gain_vector):
    return (
        field * lax.rsqrt(jnp.mean(field * field, axis=-1, keepdims=True) + EPSILON) * gain_vector
    )


VMEM = pltpu.VMEM
MESH = pl.DeviceIdType.MESH
BF16 = jnp.bfloat16
F32 = jnp.float32


def remote(src, dst, send_sem, recv_sem, partner):
    return pltpu.make_async_remote_copy(
        src_ref=src,
        dst_ref=dst,
        send_sem=send_sem,
        recv_sem=recv_sem,
        device_id=partner,
        device_id_type=MESH,
    )


def copy_of(src, dst, sem):
    return pltpu.make_async_copy(src_ref=src, dst_ref=dst, sem=sem)


def normalized(field):
    return field * lax.rsqrt(jnp.mean(field * field, axis=-1, keepdims=True) + EPSILON)


def expert_part(
    zs,
    mixed_res,
    peers,
    tp,
    z,
    allr,
    wall,
    eg,
    eu,
    ed,
    prod,
    gotc,
    summed,
    goty,
    halves,
    gotx,
    both,
    gotxx,
    gotyy,
    outz,
    gotz,
    out_ref,
    sem,
    arrived,
):
    core_peer, x_peer, y_peer, z_peer = peers
    rows = allr.shape[1] // 4
    width = allr.shape[2]
    half = width // 2
    quarter = half // 2
    copies = {}
    slot = [0]

    def send(name, src, dst, peer):
        n = slot[0]
        slot[0] += 1
        copies[name] = remote(src, dst, sem.at[0, n], sem.at[1, n], peer)
        copies[name].start()

    def block(d, rx, rc):
        return pl.ds(rc * 2 * rows + rx * rows, rows)

    def side(h):
        return pl.ds(pl.multiple_of(h * half, half), half)

    def pass_on(name, d, rx, cols, tag):
        copies[name].wait_recv()
        send(
            ("core", d, rx, tag),
            allr.at[d, block(d, rx, 0), cols],
            allr.at[d, block(d, rx, 1), cols],
            core_peer,
        )

    own = block(0, 0, 0)
    for d in range(1, zs):
        send(
            ("z", d),
            allr.at[0, own, side(tp)],
            allr.at[d, own, side(tp)],
            z_peer(-d),
        )
    send(("core", 0, 0, 0), allr.at[0, own], allr.at[0, block(0, 0, 1)], core_peer)
    send(("x", 0), allr.at[0, own], allr.at[0, block(0, 1, 0)], x_peer)
    mine, other = side(tp), side(1 - tp)
    for d in range(1, zs):
        copies["z", d].wait_recv()
        for name, peer, rx in (("x", x_peer, 1), ("y0", y_peer, 0)):
            send(
                (name, d), allr.at[d, own, mine], allr.at[d, block(d, rx, 0), mine], peer
            )
        send(
            ("core", d, 0, 0),
            allr.at[d, own, mine],
            allr.at[d, block(d, 0, 1), mine],
            core_peer,
        )
        if d == 1:
            pass_on(("x", 0), 0, 1, slice(0, width), 0)
    for move in arrived:
        move.wait()

    lane = lax.broadcasted_iota(jnp.int32, wall.shape[1:], 1)

    def expert(d):
        left = allr[d]
        gate = jnp.dot(left, eg[...], preferred_element_type=F32)
        up = jnp.dot(left, eu[...], preferred_element_type=F32)
        hidden = ((gate / (1.0 + jnp.exp(-gate))) * up).astype(BF16)
        weight = jnp.sum(jnp.where(lane == z, wall[d], 0.0), axis=1, keepdims=True)
        for n in range(width // quarter):
            cols = slice(n * quarter, (n + 1) * quarter)
            prod[d, :, cols] = (
                jnp.dot(hidden, ed[:, cols], preferred_element_type=F32) * weight
            ).astype(BF16)
        send(("rc", d), prod.at[d, 2 * rows : 4 * rows], gotc.at[d], core_peer)

    def add(a, b):
        return a.astype(F32) + b.astype(F32)

    def first_sums(d):
        copies["rc", d].wait_recv()
        summed[d] = add(prod[d, 0 : 2 * rows, :], gotc[d]).astype(BF16)
        there = pl.ds(pl.multiple_of((1 - tp) * half, half), quarter)
        send(("ry", d), summed.at[d, :, there], goty.at[d], y_peer)
        for h in range(2):
            send(
                ("rx", d, h),
                summed.at[d, rows : 2 * rows, h * half + quarter : (h + 1) * half],
                gotx.at[d, h],
                x_peer,
            )

    def second_sums(d):
        here = pl.ds(pl.multiple_of(tp * half, half), quarter)
        copies["ry", d].wait_recv()
        halves[d] = add(summed[d, :, here], goty[d]).astype(BF16)
        send(("rxx", d), halves.at[d, rows : 2 * rows], gotxx.at[d], x_peer)
        for h in range(2):
            copies["rx", d, h].wait_recv()
            both[d, h] = add(
                summed[d, 0:rows, h * half + quarter : (h + 1) * half], gotx[d, h]
            ).astype(BF16)
        send(("ryy", d), both.at[d, 1 - tp], gotyy.at[d], y_peer)

    def third_sums(d):
        copies["rxx", d].wait_recv()
        low = add(halves[d, 0:rows], gotxx[d])
        copies["ryy", d].wait_recv()
        high = add(both[d, tp], gotyy[d])
        if d == 0:
            return low, high
        outz[d, :, 0:quarter] = low.astype(BF16)
        outz[d, :, quarter:half] = high.astype(BF16)
        send(("rz", d), outz.at[d], gotz.at[d], z_peer(d))

    copies["core", 0, 0, 0].wait_recv()
    copies["core", 0, 1, 0].wait_recv()
    expert(0)
    for d in range(1, zs):
        copies["x", d].wait_recv()
        send(
            ("y1", d),
            allr.at[d, block(d, 1, 0), mine],
            allr.at[d, block(d, 1, 0), mine],
            y_peer,
        )
        send(
            ("core", d, 1, 0),
            allr.at[d, block(d, 1, 0), mine],
            allr.at[d, block(d, 1, 1), mine],
            core_peer,
        )
    first_sums(0)
    for d in range(1, zs):
        for rx in range(2):
            pass_on((f"y{rx}", d), d, rx, other, 1)
    for step in range(1, zs + 3):
        if step < zs:
            for rx in range(2):
                for tag in range(2):
                    copies["core", step, rx, tag].wait_recv()
            expert(step)
        if 0 < step - 1 < zs:
            first_sums(step - 1)
        if 0 <= step - 2 < zs:
            second_sums(step - 2)
        if 0 < step - 3 < zs:
            third_sums(step - 3)
    low, high = third_sums(0)
    for d in range(1, zs):
        copies["rz", d].wait_recv()
        low = low + gotz[d, :, 0:quarter].astype(F32)
        high = high + gotz[d, :, quarter:half].astype(F32)
    for part, value in ((0, low), (quarter, high)):
        cols = pl.ds(pl.multiple_of(tp * half + part, quarter), quarter)
        out_ref[:, part : part + quarter] = (mixed_res[:, cols] + value).astype(BF16)
    for name in copies:
        copies[name].wait_send()


def layer_kernel(
    zs,
    chunk,
    tok_hbm,
    gain_hbm,
    wq_hbm,
    wk_hbm,
    wv_hbm,
    wf_hbm,
    bias_hbm,
    kc_hbm,
    vc_hbm,
    cum_hbm,
    len_hbm,
    wo_hbm,
    gmix_hbm,
    gffn_hbm,
    eg_hbm,
    eu_hbm,
    ed_hbm,
    routes_hbm,
    shares_hbm,
    out_ref,
    nk_ref,
    nv_ref,
    gate_ref,
    mixed_res,
    tok,
    gattn,
    gmix,
    gffn,
    weights,
    wf,
    bias,
    kc,
    vc,
    cum,
    lens,
    wo,
    normed,
    xs,
    own,
    acc,
    got,
    qs,
    kn,
    vn,
    scores,
    probs,
    own_exp,
    inverse,
    outs,
    heads,
    part,
    theirs,
    local,
    xsend,
    xrecv,
    csend,
    crecv,
    fsend,
    frecv,
    tsend,
    trecv,
    zsend,
    zrecv,
    ysend,
    yrecv,
    routes,
    shares,
    marks,
    msend,
    mrecv,
    allr,
    wall,
    eg,
    eu,
    ed,
    esem,
    *expert_refs,
):
    me, tp = lax.axis_index("ep"), lax.axis_index("tp")
    place = me % SPAN
    z = me // SPAN
    core_peer = (me + 1 - 2 * (me % 2), tp)
    x_peer = (me + 2 - 4 * ((me // 2) % 2), tp)
    y_peer = (me, 1 - tp)

    def z_peer(d):
        return (((z + d + zs) % zs) * SPAN + place, tp)

    rows, width = tok.shape
    depth = wq_hbm.shape[0]
    query_cols = wq_hbm.shape[1]
    key_cols = wk_hbm.shape[1]
    slab = SPAN * depth
    total = weights.shape[1]
    chunks = total // chunk
    heads_here = query_cols // HEAD_DIM
    mine = pl.ds(pl.multiple_of(place * depth, depth), depth)
    x_place = place + 2 - 4 * ((me // 2) % 2)
    xs_rows = pl.ds(pl.multiple_of(x_place * depth, depth), depth)

    first = [
        copy_of(tok_hbm, tok, local.at[0]),
        copy_of(gain_hbm, gattn, local.at[1]),
        copy_of(wq_hbm, weights.at[mine, 0:query_cols], local.at[2]),
        copy_of(wk_hbm, weights.at[mine, query_cols : query_cols + key_cols], local.at[3]),
        copy_of(wv_hbm, weights.at[mine, query_cols + key_cols : total], local.at[4]),
        copy_of(wf_hbm, wf, local.at[5]),
        copy_of(bias_hbm, bias, local.at[6]),
        copy_of(len_hbm, lens, local.at[7]),
        copy_of(gmix_hbm, gmix, local.at[8]),
        copy_of(gffn_hbm, gffn, local.at[9]),
        copy_of(routes_hbm, routes, local.at[14]),
        copy_of(shares_hbm, shares, local.at[15]),
    ]
    later = [
        copy_of(kc_hbm, kc, local.at[10]),
        copy_of(vc_hbm, vc, local.at[11]),
        copy_of(cum_hbm, cum, local.at[12]),
        copy_of(wo_hbm, wo, local.at[13]),
    ]
    last = [
        copy_of(eg_hbm, eg, local.at[16]),
        copy_of(eu_hbm, eu, local.at[17]),
        copy_of(ed_hbm, ed, local.at[18]),
    ]
    for move in first:
        move.start()
    others = [(d, rx, rc) for d in range(zs) for rx in range(2) for rc in range(2)][1:]

    def other(d, rx, rc):
        there = place + rc * (1 - 2 * (me % 2)) + rx * (2 - 4 * ((me // 2) % 2))
        return (((z - d + zs) % zs) * SPAN + there, tp)

    partners = [other(*key) for key in others] + [y_peer]
    barrier = pltpu.get_barrier_semaphore()
    for partner in partners:
        pl.semaphore_signal(barrier, inc=1, device_id=partner, device_id_type=MESH)
    first[0].wait()
    first[1].wait()
    normed[...] = (normalized(tok[...].astype(F32)) * gattn[...]).astype(BF16)
    xs[0:rows, :] = normed[:, pl.ds(pl.multiple_of(z * slab, slab), slab)]
    for move in first[2:5]:
        move.wait()
    pl.semaphore_wait(barrier, len(partners))

    order = [chunks - 1] + list(range(chunks - 1))
    across, direct, forward, slabs, sums = {}, {}, {}, {}, {}
    for k in order:
        cols = pl.ds(k * chunk, chunk)
        view = weights.at[mine, cols]
        across[k] = remote(view, view, xsend.at[k], xrecv.at[k], x_peer)
        across[k].start()
        if k == order[0]:
            for d in range(1, zs):
                peer = z_peer(d)
                there = pl.ds(pl.multiple_of((peer[0] // SPAN) * slab, slab), slab)
                slabs[d] = remote(
                    normed.at[:, there],
                    xs.at[d * rows : (d + 1) * rows],
                    tsend.at[d],
                    trecv.at[d],
                    peer,
                )
                slabs[d].start()
    view = weights.at[mine]
    direct = remote(view, view, csend.at[0], crecv.at[0], core_peer)
    direct.start()
    for move in later + last:
        move.start()

    for move in first[5:7]:
        move.wait()
    logits = lax.dot_general(
        wf[...], normed[...], (((1,), (1,)), ((), ())), preferred_element_type=F32
    )
    row_of = lax.broadcasted_iota(jnp.int32, logits.shape, 0)
    for h in range(heads_here):
        logits = logits + jnp.where(row_of == h, bias[h], 0.0)
    gate_ref[...] = jnp.minimum(logits, 0.0) - jnp.log1p(jnp.exp(-jnp.abs(logits)))

    for move in first[10:12]:
        move.wait()
    square = lax.broadcasted_iota(jnp.int32, (rows, rows), 0) == lax.broadcasted_iota(
        jnp.int32, (rows, rows), 1
    )
    mark_lane = lax.broadcasted_iota(jnp.int32, marks.shape, 1)
    value = jnp.zeros(marks.shape, F32)
    for e in range(zs):
        line = jnp.sum(jnp.where(routes[...] == e, shares[...], 0.0), axis=0, keepdims=True)
        column = jnp.sum(jnp.where(square, line, 0.0), axis=1, keepdims=True)
        value = jnp.where(mark_lane == e, column, value)
    marks[...] = value
    wall[0, 0:rows, :] = value
    tags = {}
    for n, key in enumerate(others):
        d, rx, rc = key
        there = pl.ds(rc * 2 * rows + rx * rows, rows)
        tags[key] = remote(marks, wall.at[d, there], msend.at[n], mrecv.at[n], other(*key))
        tags[key].start()

    for d in range(1, zs):
        slabs[d].wait_recv()
    direct.wait_recv()
    for k in order:
        cols = pl.ds(k * chunk, chunk)
        across[k].wait_recv()
        view = weights.at[xs_rows, cols]
        forward[k] = remote(view, view, fsend.at[k], frecv.at[k], core_peer)
        forward[k].start()
        forward[k].wait_recv()
        product = jnp.dot(xs[...], weights[:, cols], preferred_element_type=F32)
        own[k] = product[0:rows]
        acc[k] = product[rows:].astype(BF16)
        for d in range(1, zs):
            sums[k, d] = remote(
                acc.at[k, (d - 1) * rows : d * rows],
                got.at[k, (d - 1) * rows : d * rows],
                zsend.at[k, d],
                zrecv.at[k, d],
                z_peer(-d),
            )
            sums[k, d].start()

    lane = lax.broadcasted_iota(jnp.int32, (rows, 2 * HEAD_DIM), 1)
    low = lane < HEAD_DIM
    for k in order:
        value = own[k]
        for d in range(1, zs):
            sums[k, d].wait_recv()
            value = value + got[k, (d - 1) * rows : d * rows, :].astype(F32)
        value = value.astype(BF16)
        if k == order[0]:
            nk_ref[...] = value[:, 0:key_cols]
            nv_ref[...] = value[:, key_cols:]
            kn[...] = value[:, 0:key_cols].astype(F32)
            vn[...] = value[:, key_cols:].astype(F32)
            continue
        value = value.astype(F32) * (HEAD_DIM**-0.5)
        for j in range(chunk // (2 * HEAD_DIM)):
            block = value[:, j * 2 * HEAD_DIM : (j + 1) * 2 * HEAD_DIM]
            rolled = pltpu.roll(block, HEAD_DIM, 1)
            head = (k * chunk) // HEAD_DIM + 2 * j
            if head < heads_here // 2:
                pair = (jnp.where(low, block, 0.0), jnp.where(low, rolled, 0.0))
            else:
                pair = (jnp.where(low, 0.0, rolled), jnp.where(low, 0.0, block))
            qs[pl.ds(head, rows, stride=heads_here), :] = pair[0]
            qs[pl.ds(head + 1, rows, stride=heads_here), :] = pair[1]

    for move in later:
        move.wait()
    first[7].wait()
    unroll = 4
    groups = rows // unroll
    span_len = cum.shape[2]
    places = lax.broadcasted_iota(jnp.int32, (heads_here, span_len), 1)
    lane_b = lax.broadcasted_iota(jnp.int32, gate_ref.shape, 1)

    def strip(b):
        return pl.ds(pl.multiple_of(b * heads_here, heads_here), heads_here)

    def score(g):
        for u in range(unroll):
            b = g * unroll + u
            scores[strip(b), :] = jnp.dot(
                qs[strip(b), :].astype(BF16), kc[b], preferred_element_type=F32
            )

    def soften(g):
        for u in range(unroll):
            b = g * unroll + u
            length = lens[b]
            logcum = cum[b]
            gate = jnp.sum(jnp.where(lane_b == b, gate_ref[...], 0.0), axis=1, keepdims=True)
            last = jnp.sum(jnp.where(places == length - 1, logcum, 0.0), axis=1, keepdims=True)
            mine_score = jnp.sum(qs[strip(b), :] * kn[pl.ds(b, 1), :], axis=1, keepdims=True)
            past = scores[strip(b), :] + ((last + gate) - logcum)
            past = jnp.where(places < length, past, MASKED)
            peak = jnp.maximum(jnp.max(past, axis=1, keepdims=True), mine_score)
            raised = jnp.exp(past - peak)
            mine_exp = jnp.exp(mine_score - peak)
            probs[strip(b), :] = raised.astype(BF16)
            sum_all = jnp.sum(raised, axis=1, keepdims=True) + mine_exp
            own_exp[strip(b), :] = jnp.broadcast_to(mine_exp, (heads_here, key_cols))
            inverse[strip(b), :] = jnp.broadcast_to(1.0 / sum_all, (heads_here, key_cols))

    def weigh(g):
        for u in range(unroll):
            b = g * unroll + u
            mixed = lax.dot_general(
                probs[strip(b), :],
                vc[b],
                (((1,), (1,)), ((), ())),
                preferred_element_type=F32,
            )
            mixed = mixed + own_exp[strip(b), :] * vn[pl.ds(b, 1), :]
            outs[strip(b), :] = mixed * inverse[strip(b), :]

    def turn(g, carry):
        weigh(g - 2)
        soften(g - 1)
        score(g)
        return carry

    score(0)
    soften(0)
    score(1)
    lax.fori_loop(2, groups, turn, 0)
    weigh(groups - 2)
    soften(groups - 1)
    weigh(groups - 1)

    for m in range(heads_here // 2):
        a = outs[pl.ds(2 * m, rows, stride=heads_here), :]
        b = outs[pl.ds(2 * m + 1, rows, stride=heads_here), :]
        if 2 * m < heads_here // 2:
            b = pltpu.roll(b, HEAD_DIM, 1)
        else:
            a = pltpu.roll(a, HEAD_DIM, 1)
        heads[:, m * 2 * HEAD_DIM : (m + 1) * 2 * HEAD_DIM] = jnp.where(low, a, b).astype(BF16)

    piece = 2 * chunk
    swaps = {}
    for n in range(width // piece):
        cols = pl.ds(n * piece, piece)
        part[:, cols] = jnp.dot(
            heads[...], wo[:, cols], preferred_element_type=F32
        ).astype(BF16)
        swaps[n] = remote(
            part.at[:, cols], theirs.at[:, cols], ysend.at[n], yrecv.at[n], y_peer
        )
        swaps[n].start()
    for move in first[8:10]:
        move.wait()
    for n in swaps:
        swaps[n].wait_recv()
    mix = part[...].astype(F32) + theirs[...].astype(F32)
    residual = tok[...].astype(F32) + normalized(mix) * gmix[...]
    mixed_res[...] = residual
    allr[0, 0:rows, :] = (normalized(residual) * gffn[...]).astype(BF16)
    for key in others:
        tags[key].wait_recv()
    expert_part(
        zs,
        mixed_res,
        (core_peer, x_peer, y_peer, z_peer),
        tp,
        z,
        allr,
        wall,
        eg,
        eu,
        ed,
        *expert_refs,
        out_ref,
        esem,
        last,
    )

    direct.wait_send()
    for k in order:
        across[k].wait_send()
        forward[k].wait_send()
    for d in slabs:
        slabs[d].wait_send()
    for key in sums:
        sums[key].wait_send()
    for n in swaps:
        swaps[n].wait_send()
    for key in others:
        tags[key].wait_send()


def communicate(kernel, out_shape, scratch, number, *operands, places=VMEM, limit=50):
    whole = pl.BlockSpec(memory_space=VMEM)
    many = isinstance(out_shape, tuple)
    return pl.pallas_call(
        kernel,
        out_shape=out_shape,
        in_specs=[pl.BlockSpec(memory_space=places)] * len(operands),
        out_specs=(whole,) * len(out_shape) if many else whole,
        scratch_shapes=scratch,
        compiler_params=pltpu.CompilerParams(
            collective_id=number, has_side_effects=True, vmem_limit_bytes=limit * 1024 * 1024
        ),
    )(*operands)


def body(
    tokens,
    norm_gain_attn,
    w_query,
    w_key,
    w_value,
    w_forget,
    forget_bias,
    cache_keys,
    cache_values,
    cache_logcum,
    lengths,
    w_out,
    norm_gain_mix,
    norm_gain_ffn,
    expert_gate,
    expert_up,
    expert_down,
    routes,
    route_weights,
):
    row_count = tokens.shape[0]
    model_width = tokens.shape[1]
    query_cols = w_query.shape[1]
    key_cols = w_key.shape[1]
    residual = tokens.astype(jnp.float32)
    normed = rms_scaled(residual, norm_gain_attn).astype(jnp.bfloat16)
    devices = lax.axis_size("ep")
    expert_count = devices // SPAN
    slot_count = max(2, min(row_count, 2 * row_count * TOP // expert_count))
    depth = w_query.shape[0]
    joint_cols = query_cols + 2 * key_cols
    chunk = 256
    dense = (
        slot_count == row_count
        and lax.axis_size("tp") == 2
        and devices & (devices - 1) == 0
        and depth % 128 == 0
        and joint_cols % chunk == 0
        and devices % SPAN == 0
        and key_cols == 2 * HEAD_DIM
        and 2 * key_cols == chunk
        and row_count % 8 == 0
        and model_width % (2 * chunk) == 0
    )
    if dense:
        dma = pltpu.SemaphoreType.DMA
        zs = devices // SPAN
        chunks = joint_cols // chunk
        heads_here = query_cols // HEAD_DIM
        strips = row_count * heads_here
        smem = pltpu.SMEM
        pieces = model_width // (2 * chunk)
        half = model_width // 2
        layer_out, new_keys, new_values, gate_rows = communicate(
            functools.partial(layer_kernel, zs, chunk),
            (
                jax.ShapeDtypeStruct((row_count, half), BF16),
                jax.ShapeDtypeStruct((row_count, key_cols), BF16),
                jax.ShapeDtypeStruct((row_count, key_cols), BF16),
                jax.ShapeDtypeStruct((heads_here, row_count), F32),
            ),
            [
                VMEM((row_count, model_width), F32),
                VMEM((row_count, model_width), BF16),
                VMEM((1, model_width), F32),
                VMEM((1, model_width), F32),
                VMEM((1, model_width), F32),
                VMEM((SPAN * depth, joint_cols), BF16),
                VMEM((heads_here, model_width), BF16),
                smem((heads_here,), F32),
                VMEM(cache_keys.shape, BF16),
                VMEM(cache_values.shape, BF16),
                VMEM(cache_logcum.shape, F32),
                smem((row_count,), jnp.int32),
                VMEM(w_out.shape, BF16),
                VMEM((row_count, model_width), BF16),
                VMEM((zs * row_count, SPAN * depth), BF16),
                VMEM((chunks, row_count, chunk), F32),
                VMEM((chunks, (zs - 1) * row_count, chunk), BF16),
                VMEM((chunks, (zs - 1) * row_count, chunk), BF16),
                VMEM((strips, key_cols), F32),
                VMEM((row_count, key_cols), F32),
                VMEM((row_count, key_cols), F32),
                VMEM((strips, cache_keys.shape[2]), F32),
                VMEM((strips, cache_keys.shape[2]), BF16),
                VMEM((strips, key_cols), F32),
                VMEM((strips, key_cols), F32),
                VMEM((strips, key_cols), F32),
                VMEM((row_count, query_cols), BF16),
                VMEM((row_count, model_width), BF16),
                VMEM((row_count, model_width), BF16),
                dma((19,)),
                dma((chunks,)),
                dma((chunks,)),
                dma((1,)),
                dma((1,)),
                dma((chunks,)),
                dma((chunks,)),
                dma((zs,)),
                dma((zs,)),
                dma((chunks, zs)),
                dma((chunks, zs)),
                dma((pieces,)),
                dma((pieces,)),
                VMEM((TOP, row_count), jnp.int32),
                VMEM((TOP, row_count), F32),
                VMEM((row_count, 128), F32),
                dma((devices,)),
                dma((devices,)),
                VMEM((zs, SPAN * row_count, model_width), BF16),
                VMEM((zs, SPAN * row_count, 128), F32),
                VMEM(expert_gate.shape, BF16),
                VMEM(expert_up.shape, BF16),
                VMEM(expert_down.shape, BF16),
                dma((2, zs * SPAN * SPAN)),
                VMEM((zs, SPAN * row_count, model_width), BF16),
                VMEM((zs, 2 * row_count, model_width), BF16),
                VMEM((zs, 2 * row_count, model_width), BF16),
                VMEM((zs, 2 * row_count, half // 2), BF16),
                VMEM((zs, 2 * row_count, half // 2), BF16),
                VMEM((zs, 2, row_count, half // 2), BF16),
                VMEM((zs, 2, row_count, half // 2), BF16),
                VMEM((zs, row_count, half // 2), BF16),
                VMEM((zs, row_count, half // 2), BF16),
                VMEM((zs, row_count, half), BF16),
                VMEM((zs, row_count, half), BF16),
            ],
            1,
            tokens,
            norm_gain_attn.reshape(1, -1),
            w_query,
            w_key,
            w_value,
            w_forget.T,
            forget_bias,
            cache_keys,
            cache_values,
            cache_logcum,
            lengths,
            w_out,
            norm_gain_mix.reshape(1, -1),
            norm_gain_ffn.reshape(1, -1),
            expert_gate,
            expert_up,
            expert_down,
            routes.T,
            route_weights.T,
            places=pl.ANY,
            limit=63,
        )
        return (layer_out, new_keys, new_values, gate_rows.T)
    joined = jnp.concatenate(
        (
            lax.all_gather(w_query, "ep", axis=0, tiled=True),
            lax.all_gather(w_key, "ep", axis=0, tiled=True),
            lax.all_gather(w_value, "ep", axis=0, tiled=True),
        ),
        axis=1,
    )
    projected = jnp.dot(normed, joined, preferred_element_type=jnp.float32)
    query = projected[:, :query_cols].astype(jnp.bfloat16)
    new_keys = projected[:, query_cols : query_cols + key_cols].astype(jnp.bfloat16)
    new_values = projected[:, query_cols + key_cols :].astype(jnp.bfloat16)
    new_log_gate = jax.nn.log_sigmoid(
        jnp.dot(normed, w_forget, preferred_element_type=jnp.float32) + forget_bias
    )
    local_heads = query_cols // HEAD_DIM
    local_kv = key_cols // HEAD_DIM
    group = HEAD_TOTAL // KV_HEADS
    span_len = cache_keys.shape[2]
    scale = HEAD_DIM ** (-0.5)
    query_heads = query.reshape(row_count, local_kv, group, HEAD_DIM)
    key_heads = cache_keys.reshape(row_count, local_kv, HEAD_DIM, span_len)
    value_heads = cache_values.reshape(row_count, local_kv, HEAD_DIM, span_len)
    scores = jnp.einsum(
        "bkgd,bkdl->bkgl", query_heads, key_heads, preferred_element_type=jnp.float32
    )
    scores = scores.reshape(row_count, local_heads, span_len) * scale
    own_key = new_keys.astype(jnp.float32).reshape(row_count, local_kv, 1, HEAD_DIM)
    own_score = (
        jnp.sum(query_heads.astype(jnp.float32) * own_key, axis=-1).reshape(row_count, local_heads)
        * scale
    )
    places = jnp.arange(span_len, dtype=jnp.int32)
    at_last = (places[None, :] == (lengths - 1)[:, None]).astype(jnp.float32)
    last_cum = jnp.sum(cache_logcum * at_last[:, None, :], axis=2)
    shift = (last_cum + new_log_gate)[:, :, None] - cache_logcum
    valid = (places[None, :] < lengths[:, None])[:, None, :]
    past = jnp.where(valid, scores + shift, MASKED)
    peak = jnp.maximum(jnp.max(past, axis=-1), own_score)
    past_exp = jnp.exp(past - peak[:, :, None])
    own_exp = jnp.exp(own_score - peak)
    total = jnp.sum(past_exp, axis=-1) + own_exp
    past_weight = (
        (past_exp / total[:, :, None])
        .astype(jnp.bfloat16)
        .reshape(row_count, local_kv, group, span_len)
    )
    own_weight = (
        (own_exp / total)
        .astype(jnp.bfloat16)
        .astype(jnp.float32)
        .reshape(row_count, local_kv, group)
    )
    mixed = jnp.einsum(
        "bkgl,bkdl->bkgd", past_weight, value_heads, preferred_element_type=jnp.float32
    )
    own_value = new_values.astype(jnp.float32).reshape(row_count, local_kv, 1, HEAD_DIM)
    mixed = mixed + own_weight[:, :, :, None] * own_value
    heads_out = mixed.astype(jnp.bfloat16).reshape(row_count, query_cols)
    partial_mix = (
        jnp.dot(heads_out, w_out, preferred_element_type=jnp.float32)
        .astype(jnp.bfloat16)
        .astype(jnp.float32)
    )
    mix = lax.psum(partial_mix.astype(jnp.bfloat16), "tp").astype(jnp.float32)
    mixed_res = residual + rms_scaled(mix, norm_gain_mix)
    ffn_in = rms_scaled(mixed_res, norm_gain_ffn).astype(jnp.bfloat16)
    flat_routes = routes.reshape(-1)
    expert_hits = (
        flat_routes[:, None] == jnp.arange(expert_count, dtype=jnp.int32)[None, :]
    ).astype(jnp.int32)
    earlier = jnp.cumsum(expert_hits, axis=0) - expert_hits
    slot_index = jnp.sum(earlier * expert_hits, axis=1)
    in_slot = (slot_index[:, None] == jnp.arange(slot_count, dtype=jnp.int32)[None, :]).astype(
        jnp.float32
    )
    placing = expert_hits.astype(jnp.float32)[:, :, None] * in_slot[:, None, :]
    placing = placing.reshape(row_count, TOP, expert_count * slot_count)
    selector = jnp.sum(placing, axis=1).astype(jnp.bfloat16)
    weighing = jnp.sum(placing * route_weights[:, :, None], axis=1)
    packed = jnp.einsum("ra,rd->ad", selector, ffn_in, preferred_element_type=jnp.float32).astype(
        jnp.bfloat16
    )
    outgoing = jnp.broadcast_to(
        packed.reshape(expert_count, 1, slot_count, model_width),
        (expert_count, SPAN, slot_count, model_width),
    )
    outgoing = outgoing.reshape(expert_count * SPAN, slot_count, model_width)
    arrived = lax.all_to_all(outgoing, "ep", split_axis=0, concat_axis=0, tiled=True)
    sources, slots, width = arrived.shape
    flat_rows = arrived.reshape(sources * slots, width)
    gate_part = jnp.dot(flat_rows, expert_gate, preferred_element_type=jnp.float32)
    up_part = jnp.dot(flat_rows, expert_up, preferred_element_type=jnp.float32)
    hidden = (jax.nn.silu(gate_part) * up_part).astype(jnp.bfloat16)
    expert_part = jnp.dot(hidden, expert_down, preferred_element_type=jnp.float32)
    col_share = lax.psum_scatter(
        expert_part.astype(jnp.bfloat16), "tp", scatter_dimension=1, tiled=True
    ).astype(jnp.float32)
    returned = lax.all_to_all(
        col_share.reshape(sources, slots, -1).astype(jnp.bfloat16),
        "ep",
        split_axis=0,
        concat_axis=0,
        tiled=True,
    ).astype(jnp.float32)
    col_width = returned.shape[2]
    per_expert = jnp.sum(returned.reshape(expert_count, SPAN, slot_count, col_width), axis=1)
    per_expert = per_expert.reshape(expert_count * slot_count, col_width)
    routed = jnp.dot(
        weighing, per_expert, precision=lax.Precision.HIGHEST, preferred_element_type=jnp.float32
    )
    col_start = lax.axis_index("tp") * col_width
    residual_cols = lax.dynamic_slice_in_dim(mixed_res, col_start, col_width, 1)
    layer_out = (residual_cols + routed).astype(jnp.bfloat16)
    return (layer_out, new_keys, new_values, new_log_gate)


def solution(mesh):
    placed = (
        P("ep", None),
        P(),
        P("ep", "tp"),
        P("ep", "tp"),
        P("ep", "tp"),
        P(None, "tp"),
        P("tp"),
        P("ep", "tp", None),
        P("ep", "tp", None),
        P("ep", "tp", None),
        P("ep"),
        P("tp", None),
        P(),
        P(),
        P(None, ("ep", "tp")),
        P(None, ("ep", "tp")),
        P(("ep", "tp"), None),
        P("ep", None),
        P("ep", None),
    )
    return jax.shard_map(
        body,
        mesh=mesh,
        in_specs=placed,
        out_specs=(P("ep", "tp"), P("ep", "tp"), P("ep", "tp"), P("ep", "tp")),
        check_vma=False,
    )
```

```python
import functools

import jax
import jax.numpy as jnp
from jax import lax
from jax.experimental import pallas as pl
from jax.experimental.pallas import tpu as pltpu
from jax.sharding import PartitionSpec as P

HEAD_TOTAL = 32
KV_HEADS = 4
HEAD_DIM = 64
SPAN = 4
TOP = 2


EPSILON = 1e-06
MASKED = -1e30
VMEM_LIMIT = 63 * 1024 * 1024


def rms_scaled(field, gain_vector):
    return (
        field * lax.rsqrt(jnp.mean(field * field, axis=-1, keepdims=True) + EPSILON) * gain_vector
    )


VMEM = pltpu.VMEM
MESH = pl.DeviceIdType.MESH
BF16 = jnp.bfloat16
F32 = jnp.float32


def remote(src, dst, send_sem, recv_sem, partner):
    return pltpu.make_async_remote_copy(
        src_ref=src,
        dst_ref=dst,
        send_sem=send_sem,
        recv_sem=recv_sem,
        device_id=partner,
        device_id_type=MESH,
    )


def copy_of(src, dst, sem):
    return pltpu.make_async_copy(src_ref=src, dst_ref=dst, sem=sem)


def taken(ref, sem):
    copy_of(ref, ref, sem).wait()


def normalized(field):
    return field * lax.rsqrt(jnp.mean(field * field, axis=-1, keepdims=True) + EPSILON)


def add(a, b):
    return a.astype(F32) + b.astype(F32)


def expert_part(
    zs,
    at,
    gauge,
    mixed_res,
    peers,
    tp,
    z,
    allr,
    wall,
    eg,
    eu,
    ed,
    weights_here,
    prod,
    gotc,
    summed,
    goty,
    halves,
    gotx,
    both,
    gotxx,
    gotyy,
    outz,
    gotz,
    out_ref,
):
    core_peer, x_peer, y_peer, z_peer = peers
    rows = allr.shape[1] // 4
    width = allr.shape[2]
    half = width // 2
    quarter = half // 2
    sent = {"gather": 0, "combine": 0}

    def send(stage, group, src, dst, peer):
        size = 1
        for extent in src.shape:
            size *= extent
        sent[stage] += size
        remote(src, dst, at(stage), at(group), peer).start()

    def block(rx, rc):
        return pl.ds(rc * 2 * rows + rx * rows, rows)

    def side(h):
        return pl.ds(pl.multiple_of(h * half, half), half)

    mine, other = side(tp), side(1 - tp)
    own, beside = block(0, 0), block(1, 0)
    upper, lower = pl.ds(0, 2 * rows), pl.ds(2 * rows, 2 * rows)
    for d in range(1, zs):
        send("gather", ("z", d), allr.at[0, own, mine], allr.at[d, own, mine], z_peer(-d))
    send("gather", ("core", 0), allr.at[0, own], allr.at[0, block(0, 1)], core_peer)
    send("gather", ("x", 0), allr.at[0, own], allr.at[0, beside], x_peer)

    def from_z(d):
        view = allr.at[d, own, mine]
        taken(view, at(("z", d)))
        send("gather", ("x", d), view, allr.at[d, beside, mine], x_peer)
        send("gather", ("y", d), view, view, y_peer)
        send("gather", ("core", d), view, allr.at[d, block(0, 1), mine], core_peer)

    def from_x(d):
        view = allr.at[d, beside, mine] if d else allr.at[0, beside]
        taken(view, at(("x", d)))
        if d:
            send("gather", ("y", d), view, view, y_peer)
            send("gather", ("core", d), view, allr.at[d, block(1, 1), mine], core_peer)
        else:
            send("gather", ("core", 0), view, allr.at[0, block(1, 1)], core_peer)

    def from_y(d):
        view = allr.at[d, upper, other]
        taken(view, at(("y", d)))
        send("gather", ("core", d), view, allr.at[d, lower, other], core_peer)

    lane = lax.broadcasted_iota(jnp.int32, (4 * rows, wall.shape[1]), 1)

    def expert(d):
        taken(allr.at[d, lower], at(("core", d)))
        left = allr[d]
        gate = jnp.dot(left, eg[...], preferred_element_type=F32)
        up = jnp.dot(left, eu[...], preferred_element_type=F32)
        hidden = ((gate / (1.0 + jnp.exp(-gate))) * up).astype(BF16)
        marks = wall[d * 4 * rows : (d + 1) * 4 * rows, :]
        weight = jnp.sum(jnp.where(lane == z, marks, 0.0), axis=1, keepdims=True)
        for n in range(width // quarter):
            cols = slice(n * quarter, (n + 1) * quarter)
            prod[d, :, cols] = (
                jnp.dot(hidden, ed[:, cols], preferred_element_type=F32) * weight
            ).astype(BF16)
        send("combine", ("rc", d), prod.at[d, lower], gotc.at[d], core_peer)

    def first_sums(d):
        taken(gotc.at[d], at(("rc", d)))
        summed[d] = add(prod[d, 0 : 2 * rows, :], gotc[d]).astype(BF16)
        there = pl.ds(pl.multiple_of((1 - tp) * half, half), quarter)
        send("combine", ("ry", d), summed.at[d, :, there], goty.at[d], y_peer)
        for h in range(2):
            send(
                "combine",
                ("rx", d),
                summed.at[d, pl.ds(rows, rows), pl.ds(h * half + quarter, quarter)],
                gotx.at[d, h],
                x_peer,
            )

    def second_sums(d):
        here = pl.ds(pl.multiple_of(tp * half, half), quarter)
        taken(goty.at[d], at(("ry", d)))
        halves[d] = add(summed[d, :, here], goty[d]).astype(BF16)
        send("combine", ("rxx", d), halves.at[d, pl.ds(rows, rows)], gotxx.at[d], x_peer)
        taken(gotx.at[d], at(("rx", d)))
        for h in range(2):
            both[d, h] = add(
                summed[d, 0:rows, h * half + quarter : (h + 1) * half], gotx[d, h]
            ).astype(BF16)
        send("combine", ("ryy", d), both.at[d, 1 - tp], gotyy.at[d], y_peer)

    def third_sums(d):
        taken(gotxx.at[d], at(("rxx", d)))
        low = add(halves[d, 0:rows], gotxx[d])
        taken(gotyy.at[d], at(("ryy", d)))
        high = add(both[d, tp], gotyy[d])
        if d == 0:
            return low, high
        outz[d, :, 0:quarter] = low.astype(BF16)
        outz[d, :, quarter:half] = high.astype(BF16)
        send("combine", "rz", outz.at[d], gotz.at[d], z_peer(d))

    from_z(1)
    from_x(0)
    for d in range(2, zs):
        from_z(d)
        from_x(d - 1)
    weights_here()
    from_x(zs - 1)
    from_y(1)
    expert(0)
    for d in range(1, zs):
        if d + 1 < zs:
            from_y(d + 1)
        expert(d)
        if d > 1:
            first_sums(d - 1)
    second_sums(1)
    first_sums(zs - 1)
    for d in range(2, zs):
        second_sums(d)
        if d == 2:
            first_sums(0)
        third_sums(d - 1)
    second_sums(0)
    third_sums(zs - 1)
    low, high = third_sums(0)
    taken(gotz.at[pl.ds(1, zs - 1)], at("rz"))
    for d in range(1, zs):
        low = low + gotz[d, :, 0:quarter].astype(F32)
        high = high + gotz[d, :, quarter:half].astype(F32)
    for part, value in ((0, low), (quarter, high)):
        cols = pl.ds(pl.multiple_of(tp * half + part, quarter), quarter)
        out_ref[:, part : part + quarter] = (mixed_res[:, cols] + value).astype(BF16)

    def finish():
        for stage in sent:
            units = sent[stage] // (rows * half)
            taken(gauge.at[pl.ds(0, units), pl.ds(0, rows), pl.ds(0, half)], at(stage))

    return finish


def layer_kernel(
    zs,
    chunk,
    limit,
    tok_hbm,
    gain_hbm,
    wq_hbm,
    wk_hbm,
    wv_hbm,
    wf_hbm,
    bias_hbm,
    kc_hbm,
    vc_hbm,
    cum_hbm,
    len_hbm,
    wo_hbm,
    gmix_hbm,
    gffn_hbm,
    eg_hbm,
    eu_hbm,
    ed_hbm,
    routes_hbm,
    shares_hbm,
    out_hbm,
    nk_hbm,
    nv_hbm,
    gate_hbm,
    out_ref,
    new_ref,
    gate_ref,
    mixed_res,
    tok,
    gattn,
    gains,
    weights,
    wf,
    bias,
    kc,
    vc,
    cum,
    lens,
    wo,
    normed,
    xs,
    own,
    acc,
    got,
    qs,
    kn,
    vn,
    scores,
    probs,
    own_exp,
    inverse,
    outs,
    heads,
    part,
    theirs,
    sem,
    routes,
    shares,
    marks,
    allr,
    wall,
    eg,
    eu,
    ed,
    *expert_refs,
):
    me, tp = lax.axis_index("ep"), lax.axis_index("tp")
    place = me % SPAN
    z = me // SPAN
    core_peer = (me + 1 - 2 * (me % 2), tp)
    x_peer = (me + 2 - 4 * ((me // 2) % 2), tp)
    y_peer = (me, 1 - tp)
    numbers = {}

    def at(group):
        number = numbers.setdefault(group, len(numbers))
        assert number < limit
        return sem.at[number]

    def z_peer(d):
        return (((z + d + zs) % zs) * SPAN + place, tp)

    rows, width = tok.shape
    depth = wq_hbm.shape[0]
    query_cols = wq_hbm.shape[1]
    key_cols = wk_hbm.shape[1]
    slab = SPAN * depth
    chunks = weights.shape[0]
    heads_here = query_cols // HEAD_DIM
    mine = pl.ds(pl.multiple_of(place * depth, depth), depth)
    x_place = place + 2 - 4 * ((me // 2) % 2)
    xs_rows = pl.ds(pl.multiple_of(x_place * depth, depth), depth)

    def begin(group, src, dst):
        copy_of(src, dst, at(group)).start()

    begin("tok", tok_hbm, tok)
    begin("gattn", gain_hbm, gattn)
    for k in range(chunks - 1):
        begin("w", wq_hbm.at[:, pl.ds(k * chunk, chunk)], weights.at[k, mine])
    begin("w", wk_hbm, weights.at[chunks - 1, mine, pl.ds(0, key_cols)])
    begin("w", wv_hbm, weights.at[chunks - 1, mine, pl.ds(key_cols, key_cols)])
    begin("wf", wf_hbm, wf)
    begin("bias", bias_hbm, bias)
    begin("lens", len_hbm, lens)
    begin("routes", routes_hbm, routes)
    begin("shares", shares_hbm, shares)
    begin("gains", gmix_hbm, gains.at[0])
    begin("gains", gffn_hbm, gains.at[1])

    others = [(d, rx, rc) for d in range(zs) for rx in range(2) for rc in range(2)][1:]

    def other(d, rx, rc):
        there = place + rc * (1 - 2 * (me % 2)) + rx * (2 - 4 * ((me // 2) % 2))
        return (((z - d + zs) % zs) * SPAN + there, tp)

    partners = [other(*key) for key in others] + [y_peer]
    barrier = pltpu.get_barrier_semaphore()
    for partner in partners:
        pl.semaphore_signal(barrier, inc=1, device_id=partner, device_id_type=MESH)
    taken(tok, at("tok"))
    taken(gattn, at("gattn"))
    normed[...] = (normalized(tok[...].astype(F32)) * gattn[...]).astype(BF16)
    xs[0:rows, :] = normed[:, pl.ds(pl.multiple_of(z * slab, slab), slab)]
    taken(weights.at[:, mine], at("w"))
    pl.semaphore_wait(barrier, len(partners))

    order = [chunks - 1] + list(range(chunks - 1))
    for k in order:
        view = weights.at[k, mine]
        remote(view, view, at("across"), at(("across", k)), x_peer).start()
        if k == order[0]:
            for d in range(1, zs):
                peer = z_peer(d)
                there = pl.ds(pl.multiple_of((peer[0] // SPAN) * slab, slab), slab)
                dst = xs.at[pl.ds(d * rows, rows)]
                remote(normed.at[:, there], dst, at("slabs"), at("slab"), peer).start()
    view = weights.at[:, mine]
    remote(view, view, at("directs"), at("direct"), core_peer).start()
    begin("kc", kc_hbm, kc)
    begin("cum", cum_hbm, cum)
    begin("vc", vc_hbm, vc)
    begin("wo", wo_hbm, wo)
    begin("eg", eg_hbm, eg)
    begin("eu", eu_hbm, eu)
    begin("ed", ed_hbm, ed)

    taken(wf, at("wf"))
    taken(bias, at("bias"))
    logits = lax.dot_general(
        wf[...], normed[...], (((1,), (1,)), ((), ())), preferred_element_type=F32
    )
    row_of = lax.broadcasted_iota(jnp.int32, logits.shape, 0)
    for h in range(heads_here):
        logits = logits + jnp.where(row_of == h, bias[h], 0.0)
    gate_ref[...] = jnp.minimum(logits, 0.0) - jnp.log1p(jnp.exp(-jnp.abs(logits)))

    taken(routes, at("routes"))
    taken(shares, at("shares"))
    square = lax.broadcasted_iota(jnp.int32, (rows, rows), 0) == lax.broadcasted_iota(
        jnp.int32, (rows, rows), 1
    )
    mark_lane = lax.broadcasted_iota(jnp.int32, marks.shape, 1)
    value = jnp.zeros(marks.shape, F32)
    for e in range(zs):
        line = jnp.sum(jnp.where(routes[...] == e, shares[...], 0.0), axis=0, keepdims=True)
        column = jnp.sum(jnp.where(square, line, 0.0), axis=1, keepdims=True)
        value = jnp.where(mark_lane == e, column, value)
    marks[...] = value
    wall[0:rows, :] = value
    for key in others:
        d, rx, rc = key
        there = pl.ds(d * 4 * rows + rc * 2 * rows + rx * rows, rows)
        remote(marks, wall.at[there], at("tags"), at("tag"), other(*key)).start()

    def relay(k):
        view = weights.at[k, xs_rows]
        taken(view, at(("across", k)))
        remote(view, view, at("forwards"), at(("forward", k)), core_peer).start()

    def multiply(k):
        taken(weights.at[k, xs_rows], at(("forward", k)))
        product = jnp.dot(xs[...], weights[k], preferred_element_type=F32)
        own[k] = product[0:rows]
        acc[k] = product[rows:].astype(BF16)
        for d in range(1, zs):
            view = pl.ds((d - 1) * rows, rows)
            remote(acc.at[k, view], got.at[k, view], at("sums"), at(("sum", k)), z_peer(-d)).start()

    relay(order[0])
    relay(order[1])
    taken(xs.at[pl.ds(rows, (zs - 1) * rows)], at("slab"))
    taken(view, at("direct"))
    for n, k in enumerate(order):
        multiply(k)
        if n + 2 < chunks:
            relay(order[n + 2])

    lane = lax.broadcasted_iota(jnp.int32, (rows, 2 * HEAD_DIM), 1)
    low = lane < HEAD_DIM
    group = heads_here // 2

    def collect(k):
        taken(got.at[k], at(("sum", k)))
        value = own[k]
        for d in range(1, zs):
            value = value + got[k, (d - 1) * rows : d * rows, :].astype(F32)
        value = value.astype(BF16)
        if k == order[0]:
            for n, (held, shifted, result) in enumerate(((0, kn, nk_hbm), (1, vn, nv_hbm))):
                piece = value[:, n * key_cols : (n + 1) * key_cols]
                new_ref[held] = piece
                begin("news", new_ref.at[held], result)
                shifted[0] = piece.astype(F32)
                shifted[1] = pltpu.roll(piece.astype(F32), HEAD_DIM, 1)
            begin("gates", gate_ref, gate_hbm)
            return
        value = value.astype(F32) * (HEAD_DIM**-0.5)
        for j in range(chunk // (2 * HEAD_DIM)):
            block = value[:, j * 2 * HEAD_DIM : (j + 1) * 2 * HEAD_DIM]
            kv, head = divmod((k * chunk) // HEAD_DIM + 2 * j, group)
            qs[kv, pl.ds(head, rows, stride=group), :] = block
            qs[kv, pl.ds(head + 1, rows, stride=group), :] = pltpu.roll(block, HEAD_DIM, 1)

    unroll = 8
    turns = rows // unroll
    span_len = cum.shape[2]
    places = lax.broadcasted_iota(jnp.int32, (group, span_len), 1)
    lane_b = lax.broadcasted_iota(jnp.int32, (group, rows), 1)

    def strip(b):
        return pl.ds(pl.multiple_of(b * group, group), group)

    def attend(kv):
        these = slice(kv * group, (kv + 1) * group)
        dims = slice(kv * HEAD_DIM, (kv + 1) * HEAD_DIM)

        def score(g):
            for u in range(unroll):
                b = g * unroll + u
                scores[strip(b), :] = jnp.dot(
                    qs[kv, strip(b), 0:HEAD_DIM].astype(BF16),
                    kc[b, dims, :],
                    preferred_element_type=F32,
                )

        def soften(g):
            for u in range(unroll):
                b = g * unroll + u
                length = lens[b]
                logcum = cum[b, these, :]
                gate = jnp.sum(
                    jnp.where(lane_b == b, gate_ref[these, :], 0.0), axis=1, keepdims=True
                )
                last = jnp.sum(
                    jnp.where(places == length - 1, logcum, 0.0), axis=1, keepdims=True
                )
                mine_score = jnp.sum(
                    qs[kv, strip(b), 0:HEAD_DIM] * kn[kv, pl.ds(b, 1), 0:HEAD_DIM],
                    axis=1,
                    keepdims=True,
                )
                past = scores[strip(b), :] + ((last + gate) - logcum)
                past = jnp.where(places < length, past, MASKED)
                peak = jnp.maximum(jnp.max(past, axis=1, keepdims=True), mine_score)
                raised = jnp.exp(past - peak)
                mine_exp = jnp.exp(mine_score - peak)
                probs[strip(b), :] = raised
                sum_all = jnp.sum(raised, axis=1, keepdims=True) + mine_exp
                own_exp[strip(b), :] = jnp.broadcast_to(mine_exp, (group, HEAD_DIM))
                inverse[strip(b), :] = jnp.broadcast_to(1.0 / sum_all, (group, HEAD_DIM))

        def weigh(g):
            for u in range(unroll):
                b = g * unroll + u
                mixed = lax.dot_general(
                    probs[strip(b), :].astype(BF16),
                    vc[b, dims, :],
                    (((1,), (1,)), ((), ())),
                    preferred_element_type=F32,
                )
                mixed = mixed + own_exp[strip(b), :] * vn[kv, pl.ds(b, 1), 0:HEAD_DIM]
                outs[kv, strip(b), 0:HEAD_DIM] = mixed * inverse[strip(b), :]

        def turn(g, carry):
            weigh(g - 2)
            soften(g - 1)
            score(g)
            return carry

        score(0)
        soften(0)
        score(1)
        lax.fori_loop(2, turns, turn, 0)
        weigh(turns - 2)
        soften(turns - 1)
        weigh(turns - 1)

    per_kv = (chunks - 1) // 2
    for k in order[: 1 + per_kv]:
        collect(k)
    taken(lens, at("lens"))
    taken(kc, at("kc"))
    taken(cum, at("cum"))
    taken(vc, at("vc"))
    attend(0)
    for k in order[1 + per_kv :]:
        collect(k)
    attend(1)

    for m in range(heads_here // 2):
        kv, head = divmod(2 * m, group)
        a = outs[kv, pl.ds(head, rows, stride=group), :]
        b = pltpu.roll(outs[kv, pl.ds(head + 1, rows, stride=group), :], HEAD_DIM, 1)
        heads[:, m * 2 * HEAD_DIM : (m + 1) * 2 * HEAD_DIM] = jnp.where(low, a, b).astype(BF16)

    taken(wo, at("wo"))
    piece = 2 * chunk
    for n in range(width // piece):
        cols = pl.ds(n * piece, piece)
        part[:, cols] = jnp.dot(
            heads[...], wo[:, cols], preferred_element_type=F32
        ).astype(BF16)
        remote(part.at[:, cols], theirs.at[:, cols], at("swaps"), at("swap"), y_peer).start()
    taken(gains, at("gains"))
    taken(theirs, at("swap"))
    mix = part[...].astype(F32) + theirs[...].astype(F32)
    residual = tok[...].astype(F32) + normalized(mix) * gains[0]
    mixed_res[...] = residual
    allr[0, 0:rows, :] = (normalized(residual) * gains[1]).astype(BF16)
    tagged = wall.at[pl.ds(rows, (4 * zs - 1) * rows)]
    taken(tagged, at("tag"))

    def weights_here():
        taken(eg, at("eg"))
        taken(eu, at("eu"))
        taken(ed, at("ed"))

    finish = expert_part(
        zs,
        at,
        kc,
        mixed_res,
        (core_peer, x_peer, y_peer, z_peer),
        tp,
        z,
        allr,
        wall,
        eg,
        eu,
        ed,
        weights_here,
        *expert_refs,
        out_ref,
    )
    begin("out", out_ref, out_hbm)
    finish()
    view = weights.at[:, mine]
    for group in ("across", "directs", "forwards"):
        taken(view, at(group))
    taken(xs.at[pl.ds(rows, (zs - 1) * rows)], at("slabs"))
    taken(got, at("sums"))
    taken(theirs, at("swaps"))
    taken(tagged, at("tags"))
    taken(new_ref, at("news"))
    taken(gate_ref, at("gates"))
    taken(out_ref, at("out"))
    assert len(numbers) == limit, len(numbers)


def communicate(kernel, out_shape, scratch, number, *operands):
    place = pl.BlockSpec(memory_space=pl.ANY)
    return pl.pallas_call(
        kernel,
        out_shape=out_shape,
        in_specs=[place] * len(operands),
        out_specs=(place,) * len(out_shape),
        scratch_shapes=scratch,
        compiler_params=pltpu.CompilerParams(
            collective_id=number, has_side_effects=True, vmem_limit_bytes=VMEM_LIMIT
        ),
    )(*operands)


def deliver_kernel(count, *refs):
    sources, results = refs[:count], refs[count : 2 * count]
    held, sems = refs[2 * count : 3 * count], refs[3 * count]
    moves = [copy_of(sources[n], held[n], sems.at[0, n]) for n in range(count)]
    for move in moves:
        move.start()
    outs = [copy_of(held[n], results[n], sems.at[1, n]) for n in range(count)]
    for move, out in zip(moves, outs):
        move.wait()
        out.start()
    for out in outs:
        out.wait()


def deliver(*arrays):
    count = len(arrays)
    place = pl.BlockSpec(memory_space=pl.ANY)
    return pl.pallas_call(
        functools.partial(deliver_kernel, count),
        out_shape=tuple(jax.ShapeDtypeStruct(a.shape, a.dtype) for a in arrays),
        in_specs=[place] * count,
        out_specs=(place,) * count,
        scratch_shapes=[VMEM(a.shape, a.dtype) for a in arrays]
        + [pltpu.SemaphoreType.DMA((2, count))],
        compiler_params=pltpu.CompilerParams(vmem_limit_bytes=VMEM_LIMIT),
    )(*arrays)


def body(
    tokens,
    norm_gain_attn,
    w_query,
    w_key,
    w_value,
    w_forget,
    forget_bias,
    cache_keys,
    cache_values,
    cache_logcum,
    lengths,
    w_out,
    norm_gain_mix,
    norm_gain_ffn,
    expert_gate,
    expert_up,
    expert_down,
    routes,
    route_weights,
):
    row_count = tokens.shape[0]
    model_width = tokens.shape[1]
    query_cols = w_query.shape[1]
    key_cols = w_key.shape[1]
    residual = tokens.astype(jnp.float32)
    normed = rms_scaled(residual, norm_gain_attn).astype(jnp.bfloat16)
    devices = lax.axis_size("ep")
    expert_count = devices // SPAN
    slot_count = max(2, min(row_count, 2 * row_count * TOP // expert_count))
    depth = w_query.shape[0]
    joint_cols = query_cols + 2 * key_cols
    chunk = 256
    dense = (
        slot_count == row_count
        and lax.axis_size("tp") == 2
        and devices & (devices - 1) == 0
        and depth % 128 == 0
        and joint_cols % chunk == 0
        and devices % SPAN == 0
        and key_cols == 2 * HEAD_DIM
        and 2 * key_cols == chunk
        and row_count % 8 == 0
        and model_width % (2 * chunk) == 0
    )
    if dense:
        dma = pltpu.SemaphoreType.DMA
        zs = devices // SPAN
        chunks = joint_cols // chunk
        heads_here = query_cols // HEAD_DIM
        strips = row_count * heads_here // 2
        sems = 31 + 3 * chunks + 9 * zs
        smem = pltpu.SMEM
        half = model_width // 2
        layer_out, new_keys, new_values, gate_rows = communicate(
            functools.partial(layer_kernel, zs, chunk, sems),
            (
                jax.ShapeDtypeStruct((row_count, half), BF16),
                jax.ShapeDtypeStruct((row_count, key_cols), BF16),
                jax.ShapeDtypeStruct((row_count, key_cols), BF16),
                jax.ShapeDtypeStruct((heads_here, row_count), F32),
            ),
            [
                VMEM((row_count, half), BF16),
                VMEM((2, row_count, key_cols), BF16),
                VMEM((heads_here, row_count), F32),
                VMEM((row_count, model_width), F32),
                VMEM((row_count, model_width), BF16),
                VMEM((1, model_width), F32),
                VMEM((2, 1, model_width), F32),
                VMEM((chunks, SPAN * depth, chunk), BF16),
                VMEM((heads_here, model_width), BF16),
                smem((heads_here,), F32),
                VMEM(cache_keys.shape, BF16),
                VMEM(cache_values.shape, BF16),
                VMEM(cache_logcum.shape, F32),
                smem((row_count,), jnp.int32),
                VMEM(w_out.shape, BF16),
                VMEM((row_count, model_width), BF16),
                VMEM((zs * row_count, SPAN * depth), BF16),
                VMEM((chunks, row_count, chunk), F32),
                VMEM((chunks, (zs - 1) * row_count, chunk), BF16),
                VMEM((chunks, (zs - 1) * row_count, chunk), BF16),
                VMEM((2, strips, key_cols), F32),
                VMEM((2, row_count, key_cols), F32),
                VMEM((2, row_count, key_cols), F32),
                VMEM((strips, cache_keys.shape[2]), F32),
                VMEM((strips, cache_keys.shape[2]), F32),
                VMEM((strips, HEAD_DIM), F32),
                VMEM((strips, HEAD_DIM), F32),
                VMEM((2, strips, key_cols), F32),
                VMEM((row_count, query_cols), BF16),
                VMEM((row_count, model_width), BF16),
                VMEM((row_count, model_width), BF16),
                dma((sems,)),
                VMEM((TOP, row_count), jnp.int32),
                VMEM((TOP, row_count), F32),
                VMEM((row_count, 128), F32),
                VMEM((zs, SPAN * row_count, model_width), BF16),
                VMEM((zs * SPAN * row_count, 128), F32),
                VMEM(expert_gate.shape, BF16),
                VMEM(expert_up.shape, BF16),
                VMEM(expert_down.shape, BF16),
                VMEM((zs, SPAN * row_count, model_width), BF16),
                VMEM((zs, 2 * row_count, model_width), BF16),
                VMEM((zs, 2 * row_count, model_width), BF16),
                VMEM((zs, 2 * row_count, half // 2), BF16),
                VMEM((zs, 2 * row_count, half // 2), BF16),
                VMEM((zs, 2, row_count, half // 2), BF16),
                VMEM((zs, 2, row_count, half // 2), BF16),
                VMEM((zs, row_count, half // 2), BF16),
                VMEM((zs, row_count, half // 2), BF16),
                VMEM((zs, row_count, half), BF16),
                VMEM((zs, row_count, half), BF16),
            ],
            1,
            tokens,
            norm_gain_attn.reshape(1, -1),
            w_query,
            w_key,
            w_value,
            w_forget.T,
            forget_bias,
            cache_keys,
            cache_values,
            cache_logcum,
            lengths,
            w_out,
            norm_gain_mix.reshape(1, -1),
            norm_gain_ffn.reshape(1, -1),
            expert_gate,
            expert_up,
            expert_down,
            routes.T,
            route_weights.T,
        )
        layer_out, new_keys, new_values, gate_rows = deliver(
            layer_out, new_keys, new_values, gate_rows
        )
        return (layer_out, new_keys, new_values, gate_rows.T)
    joined = jnp.concatenate(
        (
            lax.all_gather(w_query, "ep", axis=0, tiled=True),
            lax.all_gather(w_key, "ep", axis=0, tiled=True),
            lax.all_gather(w_value, "ep", axis=0, tiled=True),
        ),
        axis=1,
    )
    projected = jnp.dot(normed, joined, preferred_element_type=jnp.float32)
    query = projected[:, :query_cols].astype(jnp.bfloat16)
    new_keys = projected[:, query_cols : query_cols + key_cols].astype(jnp.bfloat16)
    new_values = projected[:, query_cols + key_cols :].astype(jnp.bfloat16)
    new_log_gate = jax.nn.log_sigmoid(
        jnp.dot(normed, w_forget, preferred_element_type=jnp.float32) + forget_bias
    )
    local_heads = query_cols // HEAD_DIM
    local_kv = key_cols // HEAD_DIM
    group = HEAD_TOTAL // KV_HEADS
    span_len = cache_keys.shape[2]
    scale = HEAD_DIM ** (-0.5)
    query_heads = query.reshape(row_count, local_kv, group, HEAD_DIM)
    key_heads = cache_keys.reshape(row_count, local_kv, HEAD_DIM, span_len)
    value_heads = cache_values.reshape(row_count, local_kv, HEAD_DIM, span_len)
    scores = jnp.einsum(
        "bkgd,bkdl->bkgl", query_heads, key_heads, preferred_element_type=jnp.float32
    )
    scores = scores.reshape(row_count, local_heads, span_len) * scale
    own_key = new_keys.astype(jnp.float32).reshape(row_count, local_kv, 1, HEAD_DIM)
    own_score = (
        jnp.sum(query_heads.astype(jnp.float32) * own_key, axis=-1).reshape(row_count, local_heads)
        * scale
    )
    places = jnp.arange(span_len, dtype=jnp.int32)
    at_last = (places[None, :] == (lengths - 1)[:, None]).astype(jnp.float32)
    last_cum = jnp.sum(cache_logcum * at_last[:, None, :], axis=2)
    shift = (last_cum + new_log_gate)[:, :, None] - cache_logcum
    valid = (places[None, :] < lengths[:, None])[:, None, :]
    past = jnp.where(valid, scores + shift, MASKED)
    peak = jnp.maximum(jnp.max(past, axis=-1), own_score)
    past_exp = jnp.exp(past - peak[:, :, None])
    own_exp = jnp.exp(own_score - peak)
    total = jnp.sum(past_exp, axis=-1) + own_exp
    past_weight = (
        (past_exp / total[:, :, None])
        .astype(jnp.bfloat16)
        .reshape(row_count, local_kv, group, span_len)
    )
    own_weight = (
        (own_exp / total)
        .astype(jnp.bfloat16)
        .astype(jnp.float32)
        .reshape(row_count, local_kv, group)
    )
    mixed = jnp.einsum(
        "bkgl,bkdl->bkgd", past_weight, value_heads, preferred_element_type=jnp.float32
    )
    own_value = new_values.astype(jnp.float32).reshape(row_count, local_kv, 1, HEAD_DIM)
    mixed = mixed + own_weight[:, :, :, None] * own_value
    heads_out = mixed.astype(jnp.bfloat16).reshape(row_count, query_cols)
    partial_mix = (
        jnp.dot(heads_out, w_out, preferred_element_type=jnp.float32)
        .astype(jnp.bfloat16)
        .astype(jnp.float32)
    )
    mix = lax.psum(partial_mix.astype(jnp.bfloat16), "tp").astype(jnp.float32)
    mixed_res = residual + rms_scaled(mix, norm_gain_mix)
    ffn_in = rms_scaled(mixed_res, norm_gain_ffn).astype(jnp.bfloat16)
    flat_routes = routes.reshape(-1)
    expert_hits = (
        flat_routes[:, None] == jnp.arange(expert_count, dtype=jnp.int32)[None, :]
    ).astype(jnp.int32)
    earlier = jnp.cumsum(expert_hits, axis=0) - expert_hits
    slot_index = jnp.sum(earlier * expert_hits, axis=1)
    in_slot = (slot_index[:, None] == jnp.arange(slot_count, dtype=jnp.int32)[None, :]).astype(
        jnp.float32
    )
    placing = expert_hits.astype(jnp.float32)[:, :, None] * in_slot[:, None, :]
    placing = placing.reshape(row_count, TOP, expert_count * slot_count)
    selector = jnp.sum(placing, axis=1).astype(jnp.bfloat16)
    weighing = jnp.sum(placing * route_weights[:, :, None], axis=1)
    packed = jnp.einsum("ra,rd->ad", selector, ffn_in, preferred_element_type=jnp.float32).astype(
        jnp.bfloat16
    )
    outgoing = jnp.broadcast_to(
        packed.reshape(expert_count, 1, slot_count, model_width),
        (expert_count, SPAN, slot_count, model_width),
    )
    outgoing = outgoing.reshape(expert_count * SPAN, slot_count, model_width)
    arrived = lax.all_to_all(outgoing, "ep", split_axis=0, concat_axis=0, tiled=True)
    sources, slots, width = arrived.shape
    flat_rows = arrived.reshape(sources * slots, width)
    gate_part = jnp.dot(flat_rows, expert_gate, preferred_element_type=jnp.float32)
    up_part = jnp.dot(flat_rows, expert_up, preferred_element_type=jnp.float32)
    hidden = (jax.nn.silu(gate_part) * up_part).astype(jnp.bfloat16)
    expert_part = jnp.dot(hidden, expert_down, preferred_element_type=jnp.float32)
    col_share = lax.psum_scatter(
        expert_part.astype(jnp.bfloat16), "tp", scatter_dimension=1, tiled=True
    ).astype(jnp.float32)
    returned = lax.all_to_all(
        col_share.reshape(sources, slots, -1).astype(jnp.bfloat16),
        "ep",
        split_axis=0,
        concat_axis=0,
        tiled=True,
    ).astype(jnp.float32)
    col_width = returned.shape[2]
    per_expert = jnp.sum(returned.reshape(expert_count, SPAN, slot_count, col_width), axis=1)
    per_expert = per_expert.reshape(expert_count * slot_count, col_width)
    routed = jnp.dot(
        weighing, per_expert, precision=lax.Precision.HIGHEST, preferred_element_type=jnp.float32
    )
    col_start = lax.axis_index("tp") * col_width
    residual_cols = lax.dynamic_slice_in_dim(mixed_res, col_start, col_width, 1)
    layer_out = (residual_cols + routed).astype(jnp.bfloat16)
    return (layer_out, new_keys, new_values, new_log_gate)


def solution(mesh):
    placed = (
        P("ep", None),
        P(),
        P("ep", "tp"),
        P("ep", "tp"),
        P("ep", "tp"),
        P(None, "tp"),
        P("tp"),
        P("ep", "tp", None),
        P("ep", "tp", None),
        P("ep", "tp", None),
        P("ep"),
        P("tp", None),
        P(),
        P(),
        P(None, ("ep", "tp")),
        P(None, ("ep", "tp")),
        P(("ep", "tp"), None),
        P("ep", None),
        P("ep", None),
    )
    return jax.shard_map(
        body,
        mesh=mesh,
        in_specs=placed,
        out_specs=(P("ep", "tp"), P("ep", "tp"), P("ep", "tp"), P("ep", "tp")),
        check_vma=False,
    )
```

```python
import functools

import jax
import jax.numpy as jnp
from jax import lax
from jax.experimental import pallas as pl
from jax.experimental.pallas import tpu as pltpu
from jax.sharding import PartitionSpec as P

HEAD_TOTAL = 32
KV_HEADS = 4
HEAD_DIM = 64
SPAN = 4
TOP = 2


EPSILON = 1e-06
MASKED = -1e30
VMEM_LIMIT = 63 * 1024 * 1024


def rms_scaled(field, gain_vector):
    return (
        field * lax.rsqrt(jnp.mean(field * field, axis=-1, keepdims=True) + EPSILON) * gain_vector
    )


VMEM = pltpu.VMEM
MESH = pl.DeviceIdType.MESH
BF16 = jnp.bfloat16
F32 = jnp.float32


def remote(src, dst, send_sem, recv_sem, partner):
    return pltpu.make_async_remote_copy(
        src_ref=src,
        dst_ref=dst,
        send_sem=send_sem,
        recv_sem=recv_sem,
        device_id=partner,
        device_id_type=MESH,
    )


def copy_of(src, dst, sem):
    return pltpu.make_async_copy(src_ref=src, dst_ref=dst, sem=sem)


def taken(ref, sem):
    copy_of(ref, ref, sem).wait()


def normalized(field):
    return field * lax.rsqrt(jnp.mean(field * field, axis=-1, keepdims=True) + EPSILON)


def add(a, b):
    return a.astype(F32) + b.astype(F32)


def expert_part(
    zs,
    at,
    gauge,
    mixed_res,
    peers,
    tp,
    z,
    allr,
    wall,
    eg,
    eu,
    ed,
    weights_here,
    prod,
    gotc,
    summed,
    goty,
    halves,
    gotx,
    both,
    gotxx,
    gotyy,
    outz,
    gotz,
    out_ref,
):
    core_peer, x_peer, y_peer, z_peer = peers
    rows = allr.shape[1] // 4
    width = allr.shape[2]
    half = width // 2
    quarter = half // 2
    sent = {"gather": 0, "combine": 0}

    def send(stage, group, src, dst, peer):
        size = 1
        for extent in src.shape:
            size *= extent
        sent[stage] += size
        remote(src, dst, at(stage), at(group), peer).start()

    def block(rx, rc):
        return pl.ds(rc * 2 * rows + rx * rows, rows)

    def cols(h, n):
        return pl.ds(pl.multiple_of(h * half + n * quarter, quarter), quarter)

    own, beside = block(0, 0), block(1, 0)
    upper, lower = pl.ds(0, 2 * rows), pl.ds(2 * rows, 2 * rows)
    for d in range(1, zs):
        for n in range(2):
            mine = cols(tp, n)
            send(
                "gather", ("z", d, n), allr.at[0, own, mine], allr.at[d, own, mine], z_peer(d)
            )
    send("gather", ("core", 0), allr.at[0, own], allr.at[0, block(0, 1)], core_peer)
    send("gather", ("x", 0), allr.at[0, own], allr.at[0, beside], x_peer)

    def from_z(d, n):
        mine = cols(tp, n)
        view = allr.at[d, own, mine]
        taken(view, at(("z", d, n)))
        send("gather", ("x", d, n), view, allr.at[d, beside, mine], x_peer)
        send("gather", ("y", d, n), view, view, y_peer)
        send("gather", ("core", d), view, allr.at[d, block(0, 1), mine], core_peer)

    def from_x(d, n):
        mine = cols(tp, n)
        view = allr.at[d, beside, mine]
        taken(view, at(("x", d, n)))
        send("gather", ("y", d, n), view, view, y_peer)
        send("gather", ("core", d), view, allr.at[d, block(1, 1), mine], core_peer)

    def from_beside():
        view = allr.at[0, beside]
        taken(view, at(("x", 0)))
        send("gather", ("core", 0), view, allr.at[0, block(1, 1)], core_peer)

    def from_y(d):
        for n in range(2):
            view = allr.at[d, upper, cols(1 - tp, n)]
            taken(view, at(("y", d, n)))
            send("gather", ("core", d), view, allr.at[d, lower, cols(1 - tp, n)], core_peer)

    square = lax.broadcasted_iota(jnp.int32, (rows, rows), 0) == lax.broadcasted_iota(
        jnp.int32, (rows, rows), 1
    )

    def column(n):
        return jnp.sum(jnp.where(square, wall[n, :, 0:rows], 0.0), axis=1, keepdims=True)

    def expert(d):
        taken(allr.at[d, lower], at(("core", d)))
        left = allr[d]
        gate = jnp.dot(left, eg[...], preferred_element_type=F32)
        up = jnp.dot(left, eu[...], preferred_element_type=F32)
        hidden = ((gate / (1.0 + jnp.exp(-gate))) * up).astype(BF16)
        weight = jnp.concatenate([column(4 * d + n) for n in range(4)], axis=0)
        for n in range(width // quarter):
            cols = slice(n * quarter, (n + 1) * quarter)
            prod[d, :, cols] = (
                jnp.dot(hidden, ed[:, cols], preferred_element_type=F32) * weight
            ).astype(BF16)
        send("combine", ("rc", d), prod.at[d, lower], gotc.at[d], core_peer)

    def first_sums(d):
        taken(gotc.at[d], at(("rc", d)))
        summed[d] = add(prod[d, 0 : 2 * rows, :], gotc[d]).astype(BF16)
        there = pl.ds(pl.multiple_of((1 - tp) * half, half), quarter)
        send("combine", ("ry", d), summed.at[d, :, there], goty.at[d], y_peer)
        for h in range(2):
            send(
                "combine",
                ("rx", d),
                summed.at[d, pl.ds(rows, rows), pl.ds(h * half + quarter, quarter)],
                gotx.at[d, h],
                x_peer,
            )

    def second_sums(d):
        here = pl.ds(pl.multiple_of(tp * half, half), quarter)
        taken(goty.at[d], at(("ry", d)))
        halves[d] = add(summed[d, :, here], goty[d]).astype(BF16)
        send("combine", ("rxx", d), halves.at[d, pl.ds(rows, rows)], gotxx.at[d], x_peer)
        taken(gotx.at[d], at(("rx", d)))
        for h in range(2):
            both[d, h] = add(
                summed[d, 0:rows, h * half + quarter : (h + 1) * half], gotx[d, h]
            ).astype(BF16)
        send("combine", ("ryy", d), both.at[d, 1 - tp], gotyy.at[d], y_peer)

    def third_sums(d):
        taken(gotxx.at[d], at(("rxx", d)))
        low = add(halves[d, 0:rows], gotxx[d])
        taken(gotyy.at[d], at(("ryy", d)))
        high = add(both[d, tp], gotyy[d])
        if d == 0:
            return low, high
        outz[d, :, 0:quarter] = low.astype(BF16)
        outz[d, :, quarter:half] = high.astype(BF16)
        send("combine", "rz", outz.at[d], gotz.at[d], z_peer(d))

    for n in range(2):
        from_z(1, n)
    from_beside()
    for d in range(2, zs):
        for n in range(2):
            from_z(d, n)
            from_x(d - 1, n)
    weights_here()
    for n in range(2):
        from_x(zs - 1, n)
    from_y(1)
    expert(0)
    for d in range(1, zs):
        if d + 1 < zs:
            from_y(d + 1)
        expert(d)
        if d > 1:
            first_sums(d - 1)
    first_sums(zs - 1)
    second_sums(1)
    for d in range(2, zs):
        second_sums(d)
        if d == 2:
            first_sums(0)
        third_sums(d - 1)
    second_sums(0)
    third_sums(zs - 1)
    low, high = third_sums(0)
    taken(gotz.at[pl.ds(1, zs - 1)], at("rz"))
    for d in range(1, zs):
        low = low + gotz[d, :, 0:quarter].astype(F32)
        high = high + gotz[d, :, quarter:half].astype(F32)
    for part, value in ((0, low), (quarter, high)):
        cols = pl.ds(pl.multiple_of(tp * half + part, quarter), quarter)
        out_ref[:, part : part + quarter] = (mixed_res[:, cols] + value).astype(BF16)

    def finish():
        for stage in sent:
            units = sent[stage] // (rows * half)
            taken(gauge.at[pl.ds(0, units), pl.ds(0, rows), pl.ds(0, half)], at(stage))

    return finish


def layer_kernel(
    zs,
    chunk,
    limit,
    tok_hbm,
    gain_hbm,
    wq_hbm,
    wk_hbm,
    wv_hbm,
    wf_hbm,
    bias_hbm,
    kc_hbm,
    vc_hbm,
    cum_hbm,
    len_hbm,
    wo_hbm,
    gmix_hbm,
    gffn_hbm,
    eg_hbm,
    eu_hbm,
    ed_hbm,
    routes_hbm,
    shares_hbm,
    out_hbm,
    nk_hbm,
    nv_hbm,
    gate_hbm,
    out_ref,
    new_ref,
    gate_ref,
    mixed_res,
    tok,
    gattn,
    gains,
    weights,
    wf,
    bias,
    kc,
    vc,
    cum,
    lens,
    wo,
    normed,
    xs,
    own,
    acc,
    got,
    qs,
    kn,
    vn,
    scores,
    probs,
    own_exp,
    inverse,
    outs,
    heads,
    part,
    theirs,
    sem,
    routes,
    shares,
    marks,
    allr,
    wall,
    eg,
    eu,
    ed,
    *expert_refs,
):
    me, tp = lax.axis_index("ep"), lax.axis_index("tp")
    place = me % SPAN
    z = me // SPAN
    core_peer = (me + 1 - 2 * (me % 2), tp)
    x_peer = (me + 2 - 4 * ((me // 2) % 2), tp)
    y_peer = (me, 1 - tp)
    numbers = {}

    def at(group):
        number = numbers.setdefault(group, len(numbers))
        assert number < limit
        return sem.at[number]

    def across_z(d):
        there = z
        for step in range(zs.bit_length()):
            if (d >> step) & 1:
                there = there + (1 << step) * (1 - 2 * ((z // (1 << step)) % 2))
        return there

    def z_peer(d):
        return (across_z(d) * SPAN + place, tp)

    rows, width = tok.shape
    depth = wq_hbm.shape[0]
    query_cols = wq_hbm.shape[1]
    key_cols = wk_hbm.shape[1]
    slab = SPAN * depth
    chunks = weights.shape[0]
    heads_here = query_cols // HEAD_DIM
    mine = pl.ds(pl.multiple_of(place * depth, depth), depth)
    x_place = place + 2 - 4 * ((me // 2) % 2)
    xs_rows = pl.ds(pl.multiple_of(x_place * depth, depth), depth)

    def begin(group, src, dst):
        copy_of(src, dst, at(group)).start()

    begin("tok", tok_hbm, tok)
    begin("gattn", gain_hbm, gattn)
    for k in range(chunks - 1):
        begin("w", wq_hbm.at[:, pl.ds(k * chunk, chunk)], weights.at[k, mine])
    begin("w", wk_hbm, weights.at[chunks - 1, mine, pl.ds(0, key_cols)])
    begin("w", wv_hbm, weights.at[chunks - 1, mine, pl.ds(key_cols, key_cols)])
    begin("wf", wf_hbm, wf)
    begin("bias", bias_hbm, bias)
    begin("lens", len_hbm, lens)
    begin("routes", routes_hbm, routes)
    begin("shares", shares_hbm, shares)
    begin("gains", gmix_hbm, gains.at[0])
    begin("gains", gffn_hbm, gains.at[1])

    others = [(d, rx, rc) for d in range(zs) for rx in range(2) for rc in range(2)][1:]

    def other(d, rx, rc):
        there = place + rc * (1 - 2 * (me % 2)) + rx * (2 - 4 * ((me // 2) % 2))
        return (across_z(d) * SPAN + there, tp)

    partners = [other(*key) for key in others] + [y_peer]
    barrier = pltpu.get_barrier_semaphore()
    for partner in partners:
        pl.semaphore_signal(barrier, inc=1, device_id=partner, device_id_type=MESH)
    taken(tok, at("tok"))
    taken(gattn, at("gattn"))
    normed[...] = (normalized(tok[...].astype(F32)) * gattn[...]).astype(BF16)
    xs[0:rows, :] = normed[:, pl.ds(pl.multiple_of(z * slab, slab), slab)]
    taken(weights.at[:, mine], at("w"))
    pl.semaphore_wait(barrier, len(partners))

    order = [chunks - 1] + list(range(chunks - 1))
    for k in order:
        view = weights.at[k, mine]
        remote(view, view, at("across"), at(("across", k)), x_peer).start()
        if k == order[0]:
            for d in range(1, zs):
                peer = z_peer(d)
                there = pl.ds(pl.multiple_of((peer[0] // SPAN) * slab, slab), slab)
                dst = xs.at[pl.ds(d * rows, rows)]
                remote(normed.at[:, there], dst, at("slabs"), at("slab"), peer).start()
    view = weights.at[:, mine]
    remote(view, view, at("directs"), at("direct"), core_peer).start()
    begin("kc", kc_hbm, kc)
    begin("cum", cum_hbm, cum)
    begin("vc", vc_hbm, vc)
    begin("wo", wo_hbm, wo)
    begin("eg", eg_hbm, eg)
    begin("eu", eu_hbm, eu)
    begin("ed", ed_hbm, ed)

    taken(wf, at("wf"))
    taken(bias, at("bias"))
    logits = lax.dot_general(
        wf[...], normed[...], (((1,), (1,)), ((), ())), preferred_element_type=F32
    )
    row_of = lax.broadcasted_iota(jnp.int32, logits.shape, 0)
    for h in range(heads_here):
        logits = logits + jnp.where(row_of == h, bias[h], 0.0)
    gate_ref[...] = jnp.minimum(logits, 0.0) - jnp.log1p(jnp.exp(-jnp.abs(logits)))

    taken(routes, at("routes"))
    taken(shares, at("shares"))
    for e in range(zs):
        line = jnp.sum(jnp.where(routes[...] == e, shares[...], 0.0), axis=0, keepdims=True)
        marks[e, :, 0:rows] = line
    for key in others:
        d, rx, rc = key
        there = other(*key)
        slot = wall.at[d * 4 + rc * 2 + rx]
        remote(marks.at[there[0] // SPAN], slot, at("tags"), at("tag"), there).start()
    wall[0] = marks[z]

    def relay(k):
        view = weights.at[k, xs_rows]
        taken(view, at(("across", k)))
        remote(view, view, at("forwards"), at(("forward", k)), core_peer).start()

    def multiply(k):
        taken(weights.at[k, xs_rows], at(("forward", k)))
        product = jnp.dot(xs[...], weights[k], preferred_element_type=F32)
        own[k] = product[0:rows]
        acc[k] = product[rows:].astype(BF16)
        for d in range(1, zs):
            view = pl.ds((d - 1) * rows, rows)
            remote(acc.at[k, view], got.at[k, view], at("sums"), at(("sum", k)), z_peer(d)).start()

    relay(order[0])
    relay(order[1])
    taken(xs.at[pl.ds(rows, (zs - 1) * rows)], at("slab"))
    taken(view, at("direct"))
    for n, k in enumerate(order):
        multiply(k)
        if n + 2 < chunks:
            relay(order[n + 2])

    lane = lax.broadcasted_iota(jnp.int32, (rows, 2 * HEAD_DIM), 1)
    low = lane < HEAD_DIM
    group = heads_here // 2

    def collect(k):
        taken(got.at[k], at(("sum", k)))
        value = own[k]
        for d in range(1, zs):
            value = value + got[k, (d - 1) * rows : d * rows, :].astype(F32)
        value = value.astype(BF16)
        if k == order[0]:
            for n, (held, shifted, result) in enumerate(((0, kn, nk_hbm), (1, vn, nv_hbm))):
                piece = value[:, n * key_cols : (n + 1) * key_cols]
                new_ref[held] = piece
                begin("news", new_ref.at[held], result)
                shifted[0] = piece.astype(F32)
                shifted[1] = pltpu.roll(piece.astype(F32), HEAD_DIM, 1)
            begin("gates", gate_ref, gate_hbm)
            return
        value = value.astype(F32) * (HEAD_DIM**-0.5)
        for j in range(chunk // (2 * HEAD_DIM)):
            block = value[:, j * 2 * HEAD_DIM : (j + 1) * 2 * HEAD_DIM]
            kv, head = divmod((k * chunk) // HEAD_DIM + 2 * j, group)
            qs[kv, pl.ds(head, rows, stride=group), :] = block
            qs[kv, pl.ds(head + 1, rows, stride=group), :] = pltpu.roll(block, HEAD_DIM, 1)

    unroll = 16
    turns = rows // unroll
    span_len = cum.shape[2]
    places = lax.broadcasted_iota(jnp.int32, (group, span_len), 1)
    lane_b = lax.broadcasted_iota(jnp.int32, (group, rows), 1)

    def strip(b):
        return pl.ds(pl.multiple_of(b * group, group), group)

    def attend(kv):
        these = slice(kv * group, (kv + 1) * group)
        dims = slice(kv * HEAD_DIM, (kv + 1) * HEAD_DIM)

        def score(g):
            for u in range(unroll):
                b = g * unroll + u
                scores[strip(b), :] = jnp.dot(
                    qs[kv, strip(b), 0:HEAD_DIM].astype(BF16),
                    kc[b, dims, :],
                    preferred_element_type=F32,
                )

        def soften(g):
            for u in range(unroll):
                b = g * unroll + u
                length = lens[b]
                logcum = cum[b, these, :]
                gate = jnp.sum(
                    jnp.where(lane_b == b, gate_ref[these, :], 0.0), axis=1, keepdims=True
                )
                last = jnp.sum(
                    jnp.where(places == length - 1, logcum, 0.0), axis=1, keepdims=True
                )
                mine_score = jnp.sum(
                    qs[kv, strip(b), 0:HEAD_DIM] * kn[kv, pl.ds(b, 1), 0:HEAD_DIM],
                    axis=1,
                    keepdims=True,
                )
                past = scores[strip(b), :] + ((last + gate) - logcum)
                past = jnp.where(places < length, past, MASKED)
                peak = jnp.maximum(jnp.max(past, axis=1, keepdims=True), mine_score)
                raised = jnp.exp(past - peak)
                mine_exp = jnp.exp(mine_score - peak)
                probs[strip(b), :] = raised
                sum_all = jnp.sum(raised, axis=1, keepdims=True) + mine_exp
                own_exp[strip(b), :] = jnp.broadcast_to(mine_exp, (group, HEAD_DIM))
                inverse[strip(b), :] = jnp.broadcast_to(1.0 / sum_all, (group, HEAD_DIM))

        def weigh(g):
            for u in range(unroll):
                b = g * unroll + u
                mixed = lax.dot_general(
                    probs[strip(b), :].astype(BF16),
                    vc[b, dims, :],
                    (((1,), (1,)), ((), ())),
                    preferred_element_type=F32,
                )
                mixed = mixed + own_exp[strip(b), :] * vn[kv, pl.ds(b, 1), 0:HEAD_DIM]
                outs[kv, strip(b), 0:HEAD_DIM] = mixed * inverse[strip(b), :]

        def turn(g, carry):
            weigh(g - 2)
            soften(g - 1)
            score(g)
            return carry

        score(0)
        soften(0)
        score(1)
        lax.fori_loop(2, turns, turn, 0)
        weigh(turns - 2)
        soften(turns - 1)
        weigh(turns - 1)

    per_kv = (chunks - 1) // 2
    for k in order[: 1 + per_kv]:
        collect(k)
    taken(lens, at("lens"))
    taken(kc, at("kc"))
    taken(cum, at("cum"))
    taken(vc, at("vc"))
    attend(0)
    for k in order[1 + per_kv :]:
        collect(k)
    attend(1)

    for m in range(heads_here // 2):
        kv, head = divmod(2 * m, group)
        a = outs[kv, pl.ds(head, rows, stride=group), :]
        b = pltpu.roll(outs[kv, pl.ds(head + 1, rows, stride=group), :], HEAD_DIM, 1)
        heads[:, m * 2 * HEAD_DIM : (m + 1) * 2 * HEAD_DIM] = jnp.where(low, a, b).astype(BF16)

    taken(wo, at("wo"))
    piece = 2 * chunk
    for n in range(width // piece):
        cols = pl.ds(n * piece, piece)
        part[:, cols] = jnp.dot(
            heads[...], wo[:, cols], preferred_element_type=F32
        ).astype(BF16)
        remote(part.at[:, cols], theirs.at[:, cols], at("swaps"), at("swap"), y_peer).start()
    taken(gains, at("gains"))
    taken(theirs, at("swap"))
    mix = part[...].astype(F32) + theirs[...].astype(F32)
    residual = tok[...].astype(F32) + normalized(mix) * gains[0]
    mixed_res[...] = residual
    allr[0, 0:rows, :] = (normalized(residual) * gains[1]).astype(BF16)
    tagged = wall.at[pl.ds(1, 4 * zs - 1)]
    taken(tagged, at("tag"))

    def weights_here():
        taken(eg, at("eg"))
        taken(eu, at("eu"))
        taken(ed, at("ed"))

    finish = expert_part(
        zs,
        at,
        kc,
        mixed_res,
        (core_peer, x_peer, y_peer, z_peer),
        tp,
        z,
        allr,
        wall,
        eg,
        eu,
        ed,
        weights_here,
        *expert_refs,
        out_ref,
    )
    begin("out", out_ref, out_hbm)
    finish()
    view = weights.at[:, mine]
    for group in ("across", "directs", "forwards"):
        taken(view, at(group))
    taken(xs.at[pl.ds(rows, (zs - 1) * rows)], at("slabs"))
    taken(got, at("sums"))
    taken(theirs, at("swaps"))
    taken(tagged, at("tags"))
    taken(new_ref, at("news"))
    taken(gate_ref, at("gates"))
    taken(out_ref, at("out"))
    assert len(numbers) == limit, len(numbers)


def communicate(kernel, out_shape, scratch, number, *operands):
    place = pl.BlockSpec(memory_space=pl.ANY)
    return pl.pallas_call(
        kernel,
        out_shape=out_shape,
        in_specs=[place] * len(operands),
        out_specs=(place,) * len(out_shape),
        scratch_shapes=scratch,
        compiler_params=pltpu.CompilerParams(
            collective_id=number, has_side_effects=True, vmem_limit_bytes=VMEM_LIMIT
        ),
    )(*operands)


def deliver_kernel(count, *refs):
    sources, results = refs[:count], refs[count : 2 * count]
    held, sems = refs[2 * count : 3 * count], refs[3 * count]
    moves = [copy_of(sources[n], held[n], sems.at[0, n]) for n in range(count)]
    for move in moves:
        move.start()
    outs = [copy_of(held[n], results[n], sems.at[1, n]) for n in range(count)]
    for move, out in zip(moves, outs):
        move.wait()
        out.start()
    for out in outs:
        out.wait()


def deliver(*arrays):
    count = len(arrays)
    place = pl.BlockSpec(memory_space=pl.ANY)
    return pl.pallas_call(
        functools.partial(deliver_kernel, count),
        out_shape=tuple(jax.ShapeDtypeStruct(a.shape, a.dtype) for a in arrays),
        in_specs=[place] * count,
        out_specs=(place,) * count,
        scratch_shapes=[VMEM(a.shape, a.dtype) for a in arrays]
        + [pltpu.SemaphoreType.DMA((2, count))],
        compiler_params=pltpu.CompilerParams(vmem_limit_bytes=VMEM_LIMIT),
    )(*arrays)


def body(
    tokens,
    norm_gain_attn,
    w_query,
    w_key,
    w_value,
    w_forget,
    forget_bias,
    cache_keys,
    cache_values,
    cache_logcum,
    lengths,
    w_out,
    norm_gain_mix,
    norm_gain_ffn,
    expert_gate,
    expert_up,
    expert_down,
    routes,
    route_weights,
):
    row_count = tokens.shape[0]
    model_width = tokens.shape[1]
    query_cols = w_query.shape[1]
    key_cols = w_key.shape[1]
    residual = tokens.astype(jnp.float32)
    normed = rms_scaled(residual, norm_gain_attn).astype(jnp.bfloat16)
    devices = lax.axis_size("ep")
    expert_count = devices // SPAN
    slot_count = max(2, min(row_count, 2 * row_count * TOP // expert_count))
    depth = w_query.shape[0]
    joint_cols = query_cols + 2 * key_cols
    chunk = 256
    dense = (
        slot_count == row_count
        and lax.axis_size("tp") == 2
        and devices & (devices - 1) == 0
        and depth % 128 == 0
        and joint_cols % chunk == 0
        and devices % SPAN == 0
        and key_cols == 2 * HEAD_DIM
        and 2 * key_cols == chunk
        and row_count % 32 == 0
        and row_count <= cache_keys.shape[1]
        and model_width <= 2 * cache_keys.shape[2]
        and model_width % (2 * chunk) == 0
    )
    if dense:
        dma = pltpu.SemaphoreType.DMA
        zs = devices // SPAN
        chunks = joint_cols // chunk
        heads_here = query_cols // HEAD_DIM
        strips = row_count * heads_here // 2
        sems = 28 + 3 * chunks + 12 * zs
        smem = pltpu.SMEM
        half = model_width // 2
        layer_out, new_keys, new_values, gate_rows = communicate(
            functools.partial(layer_kernel, zs, chunk, sems),
            (
                jax.ShapeDtypeStruct((row_count, half), BF16),
                jax.ShapeDtypeStruct((row_count, key_cols), BF16),
                jax.ShapeDtypeStruct((row_count, key_cols), BF16),
                jax.ShapeDtypeStruct((heads_here, row_count), F32),
            ),
            [
                VMEM((row_count, half), BF16),
                VMEM((2, row_count, key_cols), BF16),
                VMEM((heads_here, row_count), F32),
                VMEM((row_count, model_width), F32),
                VMEM((row_count, model_width), BF16),
                VMEM((1, model_width), F32),
                VMEM((2, 1, model_width), F32),
                VMEM((chunks, SPAN * depth, chunk), BF16),
                VMEM((heads_here, model_width), BF16),
                smem((heads_here,), F32),
                VMEM(cache_keys.shape, BF16),
                VMEM(cache_values.shape, BF16),
                VMEM(cache_logcum.shape, F32),
                smem((row_count,), jnp.int32),
                VMEM(w_out.shape, BF16),
                VMEM((row_count, model_width), BF16),
                VMEM((zs * row_count, SPAN * depth), BF16),
                VMEM((chunks, row_count, chunk), F32),
                VMEM((chunks, (zs - 1) * row_count, chunk), BF16),
                VMEM((chunks, (zs - 1) * row_count, chunk), BF16),
                VMEM((2, strips, key_cols), F32),
                VMEM((2, row_count, key_cols), F32),
                VMEM((2, row_count, key_cols), F32),
                VMEM((strips, cache_keys.shape[2]), F32),
                VMEM((strips, cache_keys.shape[2]), F32),
                VMEM((strips, HEAD_DIM), F32),
                VMEM((strips, HEAD_DIM), F32),
                VMEM((2, strips, key_cols), F32),
                VMEM((row_count, query_cols), BF16),
                VMEM((row_count, model_width), BF16),
                VMEM((row_count, model_width), BF16),
                dma((sems,)),
                VMEM((TOP, row_count), jnp.int32),
                VMEM((TOP, row_count), F32),
                VMEM((zs, 1, 128), F32),
                VMEM((zs, SPAN * row_count, model_width), BF16),
                VMEM((zs * SPAN, 1, 128), F32),
                VMEM(expert_gate.shape, BF16),
                VMEM(expert_up.shape, BF16),
                VMEM(expert_down.shape, BF16),
                VMEM((zs, SPAN * row_count, model_width), BF16),
                VMEM((zs, 2 * row_count, model_width), BF16),
                VMEM((zs, 2 * row_count, model_width), BF16),
                VMEM((zs, 2 * row_count, half // 2), BF16),
                VMEM((zs, 2 * row_count, half // 2), BF16),
                VMEM((zs, 2, row_count, half // 2), BF16),
                VMEM((zs, 2, row_count, half // 2), BF16),
                VMEM((zs, row_count, half // 2), BF16),
                VMEM((zs, row_count, half // 2), BF16),
                VMEM((zs, row_count, half), BF16),
                VMEM((zs, row_count, half), BF16),
            ],
            1,
            tokens,
            norm_gain_attn.reshape(1, -1),
            w_query,
            w_key,
            w_value,
            w_forget.T,
            forget_bias,
            cache_keys,
            cache_values,
            cache_logcum,
            lengths,
            w_out,
            norm_gain_mix.reshape(1, -1),
            norm_gain_ffn.reshape(1, -1),
            expert_gate,
            expert_up,
            expert_down,
            routes.T,
            route_weights.T,
        )
        layer_out, new_keys, new_values, gate_rows = deliver(
            layer_out, new_keys, new_values, gate_rows
        )
        return (layer_out, new_keys, new_values, gate_rows.T)
    joined = jnp.concatenate(
        (
            lax.all_gather(w_query, "ep", axis=0, tiled=True),
            lax.all_gather(w_key, "ep", axis=0, tiled=True),
            lax.all_gather(w_value, "ep", axis=0, tiled=True),
        ),
        axis=1,
    )
    projected = jnp.dot(normed, joined, preferred_element_type=jnp.float32)
    query = projected[:, :query_cols].astype(jnp.bfloat16)
    new_keys = projected[:, query_cols : query_cols + key_cols].astype(jnp.bfloat16)
    new_values = projected[:, query_cols + key_cols :].astype(jnp.bfloat16)
    new_log_gate = jax.nn.log_sigmoid(
        jnp.dot(normed, w_forget, preferred_element_type=jnp.float32) + forget_bias
    )
    local_heads = query_cols // HEAD_DIM
    local_kv = key_cols // HEAD_DIM
    group = HEAD_TOTAL // KV_HEADS
    span_len = cache_keys.shape[2]
    scale = HEAD_DIM ** (-0.5)
    query_heads = query.reshape(row_count, local_kv, group, HEAD_DIM)
    key_heads = cache_keys.reshape(row_count, local_kv, HEAD_DIM, span_len)
    value_heads = cache_values.reshape(row_count, local_kv, HEAD_DIM, span_len)
    scores = jnp.einsum(
        "bkgd,bkdl->bkgl", query_heads, key_heads, preferred_element_type=jnp.float32
    )
    scores = scores.reshape(row_count, local_heads, span_len) * scale
    own_key = new_keys.astype(jnp.float32).reshape(row_count, local_kv, 1, HEAD_DIM)
    own_score = (
        jnp.sum(query_heads.astype(jnp.float32) * own_key, axis=-1).reshape(row_count, local_heads)
        * scale
    )
    places = jnp.arange(span_len, dtype=jnp.int32)
    at_last = (places[None, :] == (lengths - 1)[:, None]).astype(jnp.float32)
    last_cum = jnp.sum(cache_logcum * at_last[:, None, :], axis=2)
    shift = (last_cum + new_log_gate)[:, :, None] - cache_logcum
    valid = (places[None, :] < lengths[:, None])[:, None, :]
    past = jnp.where(valid, scores + shift, MASKED)
    peak = jnp.maximum(jnp.max(past, axis=-1), own_score)
    past_exp = jnp.exp(past - peak[:, :, None])
    own_exp = jnp.exp(own_score - peak)
    total = jnp.sum(past_exp, axis=-1) + own_exp
    past_weight = (
        (past_exp / total[:, :, None])
        .astype(jnp.bfloat16)
        .reshape(row_count, local_kv, group, span_len)
    )
    own_weight = (
        (own_exp / total)
        .astype(jnp.bfloat16)
        .astype(jnp.float32)
        .reshape(row_count, local_kv, group)
    )
    mixed = jnp.einsum(
        "bkgl,bkdl->bkgd", past_weight, value_heads, preferred_element_type=jnp.float32
    )
    own_value = new_values.astype(jnp.float32).reshape(row_count, local_kv, 1, HEAD_DIM)
    mixed = mixed + own_weight[:, :, :, None] * own_value
    heads_out = mixed.astype(jnp.bfloat16).reshape(row_count, query_cols)
    partial_mix = (
        jnp.dot(heads_out, w_out, preferred_element_type=jnp.float32)
        .astype(jnp.bfloat16)
        .astype(jnp.float32)
    )
    mix = lax.psum(partial_mix.astype(jnp.bfloat16), "tp").astype(jnp.float32)
    mixed_res = residual + rms_scaled(mix, norm_gain_mix)
    ffn_in = rms_scaled(mixed_res, norm_gain_ffn).astype(jnp.bfloat16)
    flat_routes = routes.reshape(-1)
    expert_hits = (
        flat_routes[:, None] == jnp.arange(expert_count, dtype=jnp.int32)[None, :]
    ).astype(jnp.int32)
    earlier = jnp.cumsum(expert_hits, axis=0) - expert_hits
    slot_index = jnp.sum(earlier * expert_hits, axis=1)
    in_slot = (slot_index[:, None] == jnp.arange(slot_count, dtype=jnp.int32)[None, :]).astype(
        jnp.float32
    )
    placing = expert_hits.astype(jnp.float32)[:, :, None] * in_slot[:, None, :]
    placing = placing.reshape(row_count, TOP, expert_count * slot_count)
    selector = jnp.sum(placing, axis=1).astype(jnp.bfloat16)
    weighing = jnp.sum(placing * route_weights[:, :, None], axis=1)
    packed = jnp.einsum("ra,rd->ad", selector, ffn_in, preferred_element_type=jnp.float32).astype(
        jnp.bfloat16
    )
    outgoing = jnp.broadcast_to(
        packed.reshape(expert_count, 1, slot_count, model_width),
        (expert_count, SPAN, slot_count, model_width),
    )
    outgoing = outgoing.reshape(expert_count * SPAN, slot_count, model_width)
    arrived = lax.all_to_all(outgoing, "ep", split_axis=0, concat_axis=0, tiled=True)
    sources, slots, width = arrived.shape
    flat_rows = arrived.reshape(sources * slots, width)
    gate_part = jnp.dot(flat_rows, expert_gate, preferred_element_type=jnp.float32)
    up_part = jnp.dot(flat_rows, expert_up, preferred_element_type=jnp.float32)
    hidden = (jax.nn.silu(gate_part) * up_part).astype(jnp.bfloat16)
    expert_part = jnp.dot(hidden, expert_down, preferred_element_type=jnp.float32)
    col_share = lax.psum_scatter(
        expert_part.astype(jnp.bfloat16), "tp", scatter_dimension=1, tiled=True
    ).astype(jnp.float32)
    returned = lax.all_to_all(
        col_share.reshape(sources, slots, -1).astype(jnp.bfloat16),
        "ep",
        split_axis=0,
        concat_axis=0,
        tiled=True,
    ).astype(jnp.float32)
    col_width = returned.shape[2]
    per_expert = jnp.sum(returned.reshape(expert_count, SPAN, slot_count, col_width), axis=1)
    per_expert = per_expert.reshape(expert_count * slot_count, col_width)
    routed = jnp.dot(
        weighing, per_expert, precision=lax.Precision.HIGHEST, preferred_element_type=jnp.float32
    )
    col_start = lax.axis_index("tp") * col_width
    residual_cols = lax.dynamic_slice_in_dim(mixed_res, col_start, col_width, 1)
    layer_out = (residual_cols + routed).astype(jnp.bfloat16)
    return (layer_out, new_keys, new_values, new_log_gate)


def solution(mesh):
    placed = (
        P("ep", None),
        P(),
        P("ep", "tp"),
        P("ep", "tp"),
        P("ep", "tp"),
        P(None, "tp"),
        P("tp"),
        P("ep", "tp", None),
        P("ep", "tp", None),
        P("ep", "tp", None),
        P("ep"),
        P("tp", None),
        P(),
        P(),
        P(None, ("ep", "tp")),
        P(None, ("ep", "tp")),
        P(("ep", "tp"), None),
        P("ep", None),
        P("ep", None),
    )
    return jax.shard_map(
        body,
        mesh=mesh,
        in_specs=placed,
        out_specs=(P("ep", "tp"), P("ep", "tp"), P("ep", "tp"), P("ep", "tp")),
        check_vma=False,
    )
```

```python
import functools

import jax
import jax.numpy as jnp
from jax import lax
from jax.experimental import pallas as pl
from jax.experimental.pallas import tpu as pltpu
from jax.sharding import PartitionSpec as P

HEAD_TOTAL = 32
KV_HEADS = 4
HEAD_DIM = 64
SPAN = 4
TOP = 2


EPSILON = 1e-06
MASKED = -1e30
VMEM_LIMIT = 63 * 1024 * 1024


def rms_scaled(field, gain_vector):
    return (
        field * lax.rsqrt(jnp.mean(field * field, axis=-1, keepdims=True) + EPSILON) * gain_vector
    )


VMEM = pltpu.VMEM
MESH = pl.DeviceIdType.MESH
BF16 = jnp.bfloat16
F32 = jnp.float32


def remote(src, dst, send_sem, recv_sem, partner):
    return pltpu.make_async_remote_copy(
        src_ref=src,
        dst_ref=dst,
        send_sem=send_sem,
        recv_sem=recv_sem,
        device_id=partner,
        device_id_type=MESH,
    )


def copy_of(src, dst, sem):
    return pltpu.make_async_copy(src_ref=src, dst_ref=dst, sem=sem)


def taken(ref, sem):
    copy_of(ref, ref, sem).wait()


def normalized(field):
    return field * lax.rsqrt(jnp.mean(field * field, axis=-1, keepdims=True) + EPSILON)


def add(a, b):
    return a.astype(F32) + b.astype(F32)


def expert_part(
    zs,
    at,
    gauge,
    mixed_res,
    peers,
    tp,
    z,
    allr,
    wall,
    eg,
    eu,
    ed,
    weights_here,
    prod,
    gotc,
    summed,
    goty,
    halves,
    gotx,
    both,
    gotxx,
    gotyy,
    outz,
    gotz,
    out_ref,
):
    core_peer, x_peer, y_peer, z_peer = peers
    rows = allr.shape[1] // 4
    width = allr.shape[2]
    half = width // 2
    quarter = half // 2
    sent = {"gather": 0, "combine": 0}

    def send(stage, group, src, dst, peer):
        size = 1
        for extent in src.shape:
            size *= extent
        sent[stage] += size
        remote(src, dst, at(stage), at(group), peer).start()

    def block(rx, rc):
        return pl.ds(rc * 2 * rows + rx * rows, rows)

    def cols(h, n):
        return pl.ds(pl.multiple_of(h * half + n * quarter, quarter), quarter)

    own, beside = block(0, 0), block(1, 0)
    upper, lower = pl.ds(0, 2 * rows), pl.ds(2 * rows, 2 * rows)
    for d in range(1, zs):
        for n in range(2):
            mine = cols(tp, n)
            send(
                "gather", ("z", d, n), allr.at[0, own, mine], allr.at[d, own, mine], z_peer(d)
            )
    send("gather", ("core", 0), allr.at[0, own], allr.at[0, block(0, 1)], core_peer)
    send("gather", ("x", 0), allr.at[0, own], allr.at[0, beside], x_peer)

    def from_z(d, n):
        mine = cols(tp, n)
        view = allr.at[d, own, mine]
        taken(view, at(("z", d, n)))
        send("gather", ("x", d, n), view, allr.at[d, beside, mine], x_peer)
        send("gather", ("y", d, n), view, view, y_peer)
        send("gather", ("core", d), view, allr.at[d, block(0, 1), mine], core_peer)

    def from_x(d, n):
        mine = cols(tp, n)
        view = allr.at[d, beside, mine]
        taken(view, at(("x", d, n)))
        send("gather", ("y", d, n), view, view, y_peer)
        send("gather", ("core", d), view, allr.at[d, block(1, 1), mine], core_peer)

    def from_beside():
        view = allr.at[0, beside]
        taken(view, at(("x", 0)))
        send("gather", ("core", 0), view, allr.at[0, block(1, 1)], core_peer)

    def from_y(d):
        for n in range(2):
            view = allr.at[d, upper, cols(1 - tp, n)]
            taken(view, at(("y", d, n)))
            send("gather", ("core", d), view, allr.at[d, lower, cols(1 - tp, n)], core_peer)

    square = lax.broadcasted_iota(jnp.int32, (rows, rows), 0) == lax.broadcasted_iota(
        jnp.int32, (rows, rows), 1
    )

    def column(n):
        return jnp.sum(jnp.where(square, wall[n, :, 0:rows], 0.0), axis=1, keepdims=True)

    def expert(d):
        taken(allr.at[d, lower], at(("core", d)))
        left = allr[d]
        gate = jnp.dot(left, eg[...], preferred_element_type=F32)
        up = jnp.dot(left, eu[...], preferred_element_type=F32)
        hidden = ((gate / (1.0 + jnp.exp(-gate))) * up).astype(BF16)
        weight = jnp.concatenate([column(4 * d + n) for n in range(4)], axis=0)
        for n in range(width // quarter):
            cols = slice(n * quarter, (n + 1) * quarter)
            prod[d, :, cols] = (
                jnp.dot(hidden, ed[:, cols], preferred_element_type=F32) * weight
            ).astype(BF16)
        send("combine", ("rc", d), prod.at[d, lower], gotc.at[d], core_peer)

    def first_sums(d):
        taken(gotc.at[d], at(("rc", d)))
        summed[d] = add(prod[d, 0 : 2 * rows, :], gotc[d]).astype(BF16)
        there = pl.ds(pl.multiple_of((1 - tp) * half, half), quarter)
        send("combine", ("ry", d), summed.at[d, :, there], goty.at[d], y_peer)
        for h in range(2):
            send(
                "combine",
                ("rx", d),
                summed.at[d, pl.ds(rows, rows), pl.ds(h * half + quarter, quarter)],
                gotx.at[d, h],
                x_peer,
            )

    def second_sums(d):
        here = pl.ds(pl.multiple_of(tp * half, half), quarter)
        taken(goty.at[d], at(("ry", d)))
        halves[d] = add(summed[d, :, here], goty[d]).astype(BF16)
        send("combine", ("rxx", d), halves.at[d, pl.ds(rows, rows)], gotxx.at[d], x_peer)
        taken(gotx.at[d], at(("rx", d)))
        for h in range(2):
            both[d, h] = add(
                summed[d, 0:rows, h * half + quarter : (h + 1) * half], gotx[d, h]
            ).astype(BF16)
        send("combine", ("ryy", d), both.at[d, 1 - tp], gotyy.at[d], y_peer)

    def third_sums(d):
        taken(gotxx.at[d], at(("rxx", d)))
        low = add(halves[d, 0:rows], gotxx[d])
        taken(gotyy.at[d], at(("ryy", d)))
        high = add(both[d, tp], gotyy[d])
        if d == 0:
            return low, high
        outz[d, :, 0:quarter] = low.astype(BF16)
        outz[d, :, quarter:half] = high.astype(BF16)
        send("combine", "rz", outz.at[d], gotz.at[d], z_peer(d))

    for n in range(2):
        from_z(1, n)
    from_beside()
    for d in range(2, zs):
        for n in range(2):
            from_z(d, n)
            from_x(d - 1, n)
    weights_here()
    for n in range(2):
        from_x(zs - 1, n)
    from_y(1)
    expert(0)
    for d in range(1, zs):
        if d + 1 < zs:
            from_y(d + 1)
        expert(d)
        if d > 1:
            first_sums(d - 1)
    first_sums(zs - 1)
    second_sums(1)
    for d in range(2, zs):
        second_sums(d)
        if d == 2:
            first_sums(0)
        third_sums(d - 1)
    second_sums(0)
    third_sums(zs - 1)
    low, high = third_sums(0)
    taken(gotz.at[pl.ds(1, zs - 1)], at("rz"))
    for d in range(1, zs):
        low = low + gotz[d, :, 0:quarter].astype(F32)
        high = high + gotz[d, :, quarter:half].astype(F32)
    for part, value in ((0, low), (quarter, high)):
        cols = pl.ds(pl.multiple_of(tp * half + part, quarter), quarter)
        out_ref[:, part : part + quarter] = (mixed_res[:, cols] + value).astype(BF16)

    def finish():
        for stage in sent:
            units = sent[stage] // (rows * half)
            taken(gauge.at[pl.ds(0, units), pl.ds(0, rows), pl.ds(0, half)], at(stage))

    return finish


def layer_kernel(
    zs,
    chunk,
    limit,
    tok_hbm,
    gain_hbm,
    wq_hbm,
    wk_hbm,
    wv_hbm,
    wf_hbm,
    bias_hbm,
    kc_hbm,
    vc_hbm,
    cum_hbm,
    len_hbm,
    wo_hbm,
    gmix_hbm,
    gffn_hbm,
    eg_hbm,
    eu_hbm,
    ed_hbm,
    routes_hbm,
    shares_hbm,
    out_hbm,
    nk_hbm,
    nv_hbm,
    gate_hbm,
    out_ref,
    new_ref,
    gate_ref,
    mixed_res,
    tok,
    gattn,
    gains,
    weights,
    wf,
    bias,
    kc,
    vc,
    cum,
    lens,
    wo,
    normed,
    xs,
    own,
    acc,
    got,
    qs,
    kn,
    vn,
    scores,
    probs,
    own_exp,
    inverse,
    outs,
    heads,
    part,
    theirs,
    sem,
    routes,
    shares,
    marks,
    allr,
    wall,
    eg,
    eu,
    ed,
    *expert_refs,
):
    me, tp = lax.axis_index("ep"), lax.axis_index("tp")
    place = me % SPAN
    z = me // SPAN
    core_peer = (me + 1 - 2 * (me % 2), tp)
    x_peer = (me + 2 - 4 * ((me // 2) % 2), tp)
    y_peer = (me, 1 - tp)
    numbers = {}

    def at(group):
        number = numbers.setdefault(group, len(numbers))
        assert number < limit
        return sem.at[number]

    def across_z(d):
        there = z
        for step in range(zs.bit_length()):
            if (d >> step) & 1:
                there = there + (1 << step) * (1 - 2 * ((z // (1 << step)) % 2))
        return there

    def z_peer(d):
        return (across_z(d) * SPAN + place, tp)

    rows, width = tok.shape
    depth = wq_hbm.shape[0]
    query_cols = wq_hbm.shape[1]
    key_cols = wk_hbm.shape[1]
    slab = SPAN * depth
    chunks = weights.shape[0]
    heads_here = query_cols // HEAD_DIM
    mine = pl.ds(pl.multiple_of(place * depth, depth), depth)
    x_place = place + 2 - 4 * ((me // 2) % 2)
    xs_rows = pl.ds(pl.multiple_of(x_place * depth, depth), depth)

    def begin(group, src, dst):
        copy_of(src, dst, at(group)).start()

    begin("tok", tok_hbm, tok)
    begin("gattn", gain_hbm, gattn)
    for k in range(chunks - 1):
        begin("w", wq_hbm.at[:, pl.ds(k * chunk, chunk)], weights.at[k, mine])
    begin("w", wk_hbm, weights.at[chunks - 1, mine, pl.ds(0, key_cols)])
    begin("w", wv_hbm, weights.at[chunks - 1, mine, pl.ds(key_cols, key_cols)])
    begin("wf", wf_hbm, wf)
    begin("bias", bias_hbm, bias)
    begin("lens", len_hbm, lens)
    begin("routes", routes_hbm, routes)
    begin("shares", shares_hbm, shares)
    begin("gains", gmix_hbm, gains.at[0])
    begin("gains", gffn_hbm, gains.at[1])

    others = [(d, rx, rc) for d in range(zs) for rx in range(2) for rc in range(2)][1:]

    def other(d, rx, rc):
        there = place + rc * (1 - 2 * (me % 2)) + rx * (2 - 4 * ((me // 2) % 2))
        return (across_z(d) * SPAN + there, tp)

    partners = [other(*key) for key in others] + [y_peer]
    barrier = pltpu.get_barrier_semaphore()
    for partner in partners:
        pl.semaphore_signal(barrier, inc=1, device_id=partner, device_id_type=MESH)
    taken(tok, at("tok"))
    taken(gattn, at("gattn"))
    normed[...] = (normalized(tok[...].astype(F32)) * gattn[...]).astype(BF16)
    xs[0:rows, :] = normed[:, pl.ds(pl.multiple_of(z * slab, slab), slab)]
    taken(weights.at[:, mine], at("w"))
    pl.semaphore_wait(barrier, len(partners))

    order = [chunks - 1] + list(range(chunks - 1))
    for k in order:
        view = weights.at[k, mine]
        remote(view, view, at("across"), at(("across", k)), x_peer).start()
        if k == order[0]:
            for d in range(1, zs):
                peer = z_peer(d)
                there = pl.ds(pl.multiple_of((peer[0] // SPAN) * slab, slab), slab)
                dst = xs.at[pl.ds(d * rows, rows)]
                remote(normed.at[:, there], dst, at("slabs"), at("slab"), peer).start()
    view = weights.at[:, mine]
    remote(view, view, at("directs"), at("direct"), core_peer).start()
    begin("kc", kc_hbm, kc)
    begin("cum", cum_hbm, cum)
    begin("vc", vc_hbm, vc)
    begin("wo", wo_hbm, wo)
    begin("eg", eg_hbm, eg)
    begin("eu", eu_hbm, eu)
    begin("ed", ed_hbm, ed)

    taken(wf, at("wf"))
    taken(bias, at("bias"))
    logits = lax.dot_general(
        wf[...], normed[...], (((1,), (1,)), ((), ())), preferred_element_type=F32
    )
    row_of = lax.broadcasted_iota(jnp.int32, logits.shape, 0)
    for h in range(heads_here):
        logits = logits + jnp.where(row_of == h, bias[h], 0.0)
    gate_ref[...] = jnp.minimum(logits, 0.0) - jnp.log1p(jnp.exp(-jnp.abs(logits)))

    taken(routes, at("routes"))
    taken(shares, at("shares"))
    for e in range(zs):
        line = jnp.sum(jnp.where(routes[...] == e, shares[...], 0.0), axis=0, keepdims=True)
        marks[e, :, 0:rows] = line
    for key in others:
        d, rx, rc = key
        there = other(*key)
        slot = wall.at[d * 4 + rc * 2 + rx]
        remote(marks.at[there[0] // SPAN], slot, at("tags"), at("tag"), there).start()
    wall[0] = marks[z]

    def relay(k):
        view = weights.at[k, xs_rows]
        taken(view, at(("across", k)))
        remote(view, view, at("forwards"), at(("forward", k)), core_peer).start()

    def multiply(k):
        taken(weights.at[k, xs_rows], at(("forward", k)))
        product = jnp.dot(xs[...], weights[k], preferred_element_type=F32)
        own[k] = product[0:rows]
        acc[k] = product[rows:].astype(BF16)
        for d in range(1, zs):
            view = pl.ds((d - 1) * rows, rows)
            remote(acc.at[k, view], got.at[k, view], at("sums"), at(("sum", k)), z_peer(d)).start()

    relay(order[0])
    taken(xs.at[pl.ds(rows, (zs - 1) * rows)], at("slab"))
    taken(view, at("direct"))
    for n, k in enumerate(order):
        if n + 1 < chunks:
            relay(order[n + 1])
        multiply(k)

    lane = lax.broadcasted_iota(jnp.int32, (rows, 2 * HEAD_DIM), 1)
    low = lane < HEAD_DIM
    group = heads_here // 2

    def collect(k):
        taken(got.at[k], at(("sum", k)))
        value = own[k]
        for d in range(1, zs):
            value = value + got[k, (d - 1) * rows : d * rows, :].astype(F32)
        value = value.astype(BF16)
        if k == order[0]:
            for n, (held, shifted, result) in enumerate(((0, kn, nk_hbm), (1, vn, nv_hbm))):
                piece = value[:, n * key_cols : (n + 1) * key_cols]
                new_ref[held] = piece
                begin("news", new_ref.at[held], result)
                shifted[0] = piece.astype(F32)
                shifted[1] = pltpu.roll(piece.astype(F32), HEAD_DIM, 1)
            begin("gates", gate_ref, gate_hbm)
            return
        value = value.astype(F32) * (HEAD_DIM**-0.5)
        for j in range(chunk // (2 * HEAD_DIM)):
            block = value[:, j * 2 * HEAD_DIM : (j + 1) * 2 * HEAD_DIM]
            kv, head = divmod((k * chunk) // HEAD_DIM + 2 * j, group)
            qs[kv, pl.ds(head, rows, stride=group), :] = block
            qs[kv, pl.ds(head + 1, rows, stride=group), :] = pltpu.roll(block, HEAD_DIM, 1)

    unroll = 16
    turns = rows // unroll
    span_len = cum.shape[2]
    places = lax.broadcasted_iota(jnp.int32, (group, span_len), 1)
    lane_b = lax.broadcasted_iota(jnp.int32, (group, rows), 1)

    def strip(b):
        return pl.ds(pl.multiple_of(b * group, group), group)

    def attend(kv):
        these = slice(kv * group, (kv + 1) * group)
        dims = slice(kv * HEAD_DIM, (kv + 1) * HEAD_DIM)

        def score(g):
            for u in range(unroll):
                b = g * unroll + u
                scores[strip(b), :] = jnp.dot(
                    qs[kv, strip(b), 0:HEAD_DIM].astype(BF16),
                    kc[b, dims, :],
                    preferred_element_type=F32,
                )

        def soften(g):
            for u in range(unroll):
                b = g * unroll + u
                length = lens[b]
                logcum = cum[b, these, :]
                gate = jnp.sum(
                    jnp.where(lane_b == b, gate_ref[these, :], 0.0), axis=1, keepdims=True
                )
                last = jnp.sum(
                    jnp.where(places == length - 1, logcum, 0.0), axis=1, keepdims=True
                )
                mine_score = jnp.sum(
                    qs[kv, strip(b), 0:HEAD_DIM] * kn[kv, pl.ds(b, 1), 0:HEAD_DIM],
                    axis=1,
                    keepdims=True,
                )
                past = scores[strip(b), :] + ((last + gate) - logcum)
                past = jnp.where(places < length, past, MASKED)
                peak = jnp.maximum(jnp.max(past, axis=1, keepdims=True), mine_score)
                raised = jnp.exp(past - peak)
                mine_exp = jnp.exp(mine_score - peak)
                probs[strip(b), :] = raised
                sum_all = jnp.sum(raised, axis=1, keepdims=True) + mine_exp
                own_exp[strip(b), :] = jnp.broadcast_to(mine_exp, (group, HEAD_DIM))
                inverse[strip(b), :] = jnp.broadcast_to(1.0 / sum_all, (group, HEAD_DIM))

        def weigh(g):
            for u in range(unroll):
                b = g * unroll + u
                mixed = lax.dot_general(
                    probs[strip(b), :].astype(BF16),
                    vc[b, dims, :],
                    (((1,), (1,)), ((), ())),
                    preferred_element_type=F32,
                )
                mixed = mixed + own_exp[strip(b), :] * vn[kv, pl.ds(b, 1), 0:HEAD_DIM]
                outs[kv, strip(b), 0:HEAD_DIM] = mixed * inverse[strip(b), :]

        def turn(g, carry):
            weigh(g - 2)
            soften(g - 1)
            score(g)
            return carry

        score(0)
        soften(0)
        score(1)
        lax.fori_loop(2, turns, turn, 0)
        weigh(turns - 2)
        soften(turns - 1)
        weigh(turns - 1)

    per_kv = (chunks - 1) // 2
    for k in order[: 1 + per_kv]:
        collect(k)
    taken(lens, at("lens"))
    taken(kc, at("kc"))
    taken(cum, at("cum"))
    taken(vc, at("vc"))
    attend(0)
    for k in order[1 + per_kv :]:
        collect(k)
    attend(1)

    for m in range(heads_here // 2):
        kv, head = divmod(2 * m, group)
        a = outs[kv, pl.ds(head, rows, stride=group), :]
        b = pltpu.roll(outs[kv, pl.ds(head + 1, rows, stride=group), :], HEAD_DIM, 1)
        heads[:, m * 2 * HEAD_DIM : (m + 1) * 2 * HEAD_DIM] = jnp.where(low, a, b).astype(BF16)

    taken(wo, at("wo"))
    piece = 2 * chunk
    for n in range(width // piece):
        cols = pl.ds(n * piece, piece)
        part[:, cols] = jnp.dot(
            heads[...], wo[:, cols], preferred_element_type=F32
        ).astype(BF16)
        remote(part.at[:, cols], theirs.at[:, cols], at("swaps"), at("swap"), y_peer).start()
    taken(gains, at("gains"))
    taken(theirs, at("swap"))
    mix = part[...].astype(F32) + theirs[...].astype(F32)
    residual = tok[...].astype(F32) + normalized(mix) * gains[0]
    mixed_res[...] = residual
    allr[0, 0:rows, :] = (normalized(residual) * gains[1]).astype(BF16)
    tagged = wall.at[pl.ds(1, 4 * zs - 1)]
    taken(tagged, at("tag"))

    def weights_here():
        taken(eg, at("eg"))
        taken(eu, at("eu"))
        taken(ed, at("ed"))

    finish = expert_part(
        zs,
        at,
        kc,
        mixed_res,
        (core_peer, x_peer, y_peer, z_peer),
        tp,
        z,
        allr,
        wall,
        eg,
        eu,
        ed,
        weights_here,
        *expert_refs,
        out_ref,
    )
    begin("out", out_ref, out_hbm)
    finish()
    view = weights.at[:, mine]
    for group in ("across", "directs", "forwards"):
        taken(view, at(group))
    taken(xs.at[pl.ds(rows, (zs - 1) * rows)], at("slabs"))
    taken(got, at("sums"))
    taken(theirs, at("swaps"))
    taken(tagged, at("tags"))
    taken(new_ref, at("news"))
    taken(gate_ref, at("gates"))
    taken(out_ref, at("out"))
    assert len(numbers) == limit, len(numbers)


def communicate(kernel, out_shape, scratch, number, *operands):
    place = pl.BlockSpec(memory_space=pl.ANY)
    return pl.pallas_call(
        kernel,
        out_shape=out_shape,
        in_specs=[place] * len(operands),
        out_specs=(place,) * len(out_shape),
        scratch_shapes=scratch,
        compiler_params=pltpu.CompilerParams(
            collective_id=number, has_side_effects=True, vmem_limit_bytes=VMEM_LIMIT
        ),
    )(*operands)


def deliver_kernel(count, *refs):
    sources, results = refs[:count], refs[count : 2 * count]
    held, sems = refs[2 * count : 3 * count], refs[3 * count]
    moves = [copy_of(sources[n], held[n], sems.at[0, n]) for n in range(count)]
    for move in moves:
        move.start()
    outs = [copy_of(held[n], results[n], sems.at[1, n]) for n in range(count)]
    for move, out in zip(moves, outs):
        move.wait()
        out.start()
    for out in outs:
        out.wait()


def deliver(*arrays):
    count = len(arrays)
    place = pl.BlockSpec(memory_space=pl.ANY)
    return pl.pallas_call(
        functools.partial(deliver_kernel, count),
        out_shape=tuple(jax.ShapeDtypeStruct(a.shape, a.dtype) for a in arrays),
        in_specs=[place] * count,
        out_specs=(place,) * count,
        scratch_shapes=[VMEM(a.shape, a.dtype) for a in arrays]
        + [pltpu.SemaphoreType.DMA((2, count))],
        compiler_params=pltpu.CompilerParams(vmem_limit_bytes=VMEM_LIMIT),
    )(*arrays)


def body(
    tokens,
    norm_gain_attn,
    w_query,
    w_key,
    w_value,
    w_forget,
    forget_bias,
    cache_keys,
    cache_values,
    cache_logcum,
    lengths,
    w_out,
    norm_gain_mix,
    norm_gain_ffn,
    expert_gate,
    expert_up,
    expert_down,
    routes,
    route_weights,
):
    row_count = tokens.shape[0]
    model_width = tokens.shape[1]
    query_cols = w_query.shape[1]
    key_cols = w_key.shape[1]
    residual = tokens.astype(jnp.float32)
    normed = rms_scaled(residual, norm_gain_attn).astype(jnp.bfloat16)
    devices = lax.axis_size("ep")
    expert_count = devices // SPAN
    slot_count = max(2, min(row_count, 2 * row_count * TOP // expert_count))
    depth = w_query.shape[0]
    joint_cols = query_cols + 2 * key_cols
    chunk = 256
    dense = (
        slot_count == row_count
        and lax.axis_size("tp") == 2
        and devices & (devices - 1) == 0
        and depth % 128 == 0
        and joint_cols % chunk == 0
        and devices % SPAN == 0
        and key_cols == 2 * HEAD_DIM
        and 2 * key_cols == chunk
        and row_count % 32 == 0
        and row_count <= cache_keys.shape[1]
        and model_width <= 2 * cache_keys.shape[2]
        and model_width % (2 * chunk) == 0
    )
    if dense:
        dma = pltpu.SemaphoreType.DMA
        zs = devices // SPAN
        chunks = joint_cols // chunk
        heads_here = query_cols // HEAD_DIM
        strips = row_count * heads_here // 2
        sems = 28 + 3 * chunks + 12 * zs
        smem = pltpu.SMEM
        half = model_width // 2
        layer_out, new_keys, new_values, gate_rows = communicate(
            functools.partial(layer_kernel, zs, chunk, sems),
            (
                jax.ShapeDtypeStruct((row_count, half), BF16),
                jax.ShapeDtypeStruct((row_count, key_cols), BF16),
                jax.ShapeDtypeStruct((row_count, key_cols), BF16),
                jax.ShapeDtypeStruct((heads_here, row_count), F32),
            ),
            [
                VMEM((row_count, half), BF16),
                VMEM((2, row_count, key_cols), BF16),
                VMEM((heads_here, row_count), F32),
                VMEM((row_count, model_width), F32),
                VMEM((row_count, model_width), BF16),
                VMEM((1, model_width), F32),
                VMEM((2, 1, model_width), F32),
                VMEM((chunks, SPAN * depth, chunk), BF16),
                VMEM((heads_here, model_width), BF16),
                smem((heads_here,), F32),
                VMEM(cache_keys.shape, BF16),
                VMEM(cache_values.shape, BF16),
                VMEM(cache_logcum.shape, F32),
                smem((row_count,), jnp.int32),
                VMEM(w_out.shape, BF16),
                VMEM((row_count, model_width), BF16),
                VMEM((zs * row_count, SPAN * depth), BF16),
                VMEM((chunks, row_count, chunk), F32),
                VMEM((chunks, (zs - 1) * row_count, chunk), BF16),
                VMEM((chunks, (zs - 1) * row_count, chunk), BF16),
                VMEM((2, strips, key_cols), F32),
                VMEM((2, row_count, key_cols), F32),
                VMEM((2, row_count, key_cols), F32),
                VMEM((strips, cache_keys.shape[2]), F32),
                VMEM((strips, cache_keys.shape[2]), F32),
                VMEM((strips, HEAD_DIM), F32),
                VMEM((strips, HEAD_DIM), F32),
                VMEM((2, strips, key_cols), F32),
                VMEM((row_count, query_cols), BF16),
                VMEM((row_count, model_width), BF16),
                VMEM((row_count, model_width), BF16),
                dma((sems,)),
                VMEM((TOP, row_count), jnp.int32),
                VMEM((TOP, row_count), F32),
                VMEM((zs, 1, 128), F32),
                VMEM((zs, SPAN * row_count, model_width), BF16),
                VMEM((zs * SPAN, 1, 128), F32),
                VMEM(expert_gate.shape, BF16),
                VMEM(expert_up.shape, BF16),
                VMEM(expert_down.shape, BF16),
                VMEM((zs, SPAN * row_count, model_width), BF16),
                VMEM((zs, 2 * row_count, model_width), BF16),
                VMEM((zs, 2 * row_count, model_width), BF16),
                VMEM((zs, 2 * row_count, half // 2), BF16),
                VMEM((zs, 2 * row_count, half // 2), BF16),
                VMEM((zs, 2, row_count, half // 2), BF16),
                VMEM((zs, 2, row_count, half // 2), BF16),
                VMEM((zs, row_count, half // 2), BF16),
                VMEM((zs, row_count, half // 2), BF16),
                VMEM((zs, row_count, half), BF16),
                VMEM((zs, row_count, half), BF16),
            ],
            1,
            tokens,
            norm_gain_attn.reshape(1, -1),
            w_query,
            w_key,
            w_value,
            w_forget.T,
            forget_bias,
            cache_keys,
            cache_values,
            cache_logcum,
            lengths,
            w_out,
            norm_gain_mix.reshape(1, -1),
            norm_gain_ffn.reshape(1, -1),
            expert_gate,
            expert_up,
            expert_down,
            routes.T,
            route_weights.T,
        )
        layer_out, new_keys, new_values, gate_rows = deliver(
            layer_out, new_keys, new_values, gate_rows
        )
        return (layer_out, new_keys, new_values, gate_rows.T)
    joined = jnp.concatenate(
        (
            lax.all_gather(w_query, "ep", axis=0, tiled=True),
            lax.all_gather(w_key, "ep", axis=0, tiled=True),
            lax.all_gather(w_value, "ep", axis=0, tiled=True),
        ),
        axis=1,
    )
    projected = jnp.dot(normed, joined, preferred_element_type=jnp.float32)
    query = projected[:, :query_cols].astype(jnp.bfloat16)
    new_keys = projected[:, query_cols : query_cols + key_cols].astype(jnp.bfloat16)
    new_values = projected[:, query_cols + key_cols :].astype(jnp.bfloat16)
    new_log_gate = jax.nn.log_sigmoid(
        jnp.dot(normed, w_forget, preferred_element_type=jnp.float32) + forget_bias
    )
    local_heads = query_cols // HEAD_DIM
    local_kv = key_cols // HEAD_DIM
    group = HEAD_TOTAL // KV_HEADS
    span_len = cache_keys.shape[2]
    scale = HEAD_DIM ** (-0.5)
    query_heads = query.reshape(row_count, local_kv, group, HEAD_DIM)
    key_heads = cache_keys.reshape(row_count, local_kv, HEAD_DIM, span_len)
    value_heads = cache_values.reshape(row_count, local_kv, HEAD_DIM, span_len)
    scores = jnp.einsum(
        "bkgd,bkdl->bkgl", query_heads, key_heads, preferred_element_type=jnp.float32
    )
    scores = scores.reshape(row_count, local_heads, span_len) * scale
    own_key = new_keys.astype(jnp.float32).reshape(row_count, local_kv, 1, HEAD_DIM)
    own_score = (
        jnp.sum(query_heads.astype(jnp.float32) * own_key, axis=-1).reshape(row_count, local_heads)
        * scale
    )
    places = jnp.arange(span_len, dtype=jnp.int32)
    at_last = (places[None, :] == (lengths - 1)[:, None]).astype(jnp.float32)
    last_cum = jnp.sum(cache_logcum * at_last[:, None, :], axis=2)
    shift = (last_cum + new_log_gate)[:, :, None] - cache_logcum
    valid = (places[None, :] < lengths[:, None])[:, None, :]
    past = jnp.where(valid, scores + shift, MASKED)
    peak = jnp.maximum(jnp.max(past, axis=-1), own_score)
    past_exp = jnp.exp(past - peak[:, :, None])
    own_exp = jnp.exp(own_score - peak)
    total = jnp.sum(past_exp, axis=-1) + own_exp
    past_weight = (
        (past_exp / total[:, :, None])
        .astype(jnp.bfloat16)
        .reshape(row_count, local_kv, group, span_len)
    )
    own_weight = (
        (own_exp / total)
        .astype(jnp.bfloat16)
        .astype(jnp.float32)
        .reshape(row_count, local_kv, group)
    )
    mixed = jnp.einsum(
        "bkgl,bkdl->bkgd", past_weight, value_heads, preferred_element_type=jnp.float32
    )
    own_value = new_values.astype(jnp.float32).reshape(row_count, local_kv, 1, HEAD_DIM)
    mixed = mixed + own_weight[:, :, :, None] * own_value
    heads_out = mixed.astype(jnp.bfloat16).reshape(row_count, query_cols)
    partial_mix = (
        jnp.dot(heads_out, w_out, preferred_element_type=jnp.float32)
        .astype(jnp.bfloat16)
        .astype(jnp.float32)
    )
    mix = lax.psum(partial_mix.astype(jnp.bfloat16), "tp").astype(jnp.float32)
    mixed_res = residual + rms_scaled(mix, norm_gain_mix)
    ffn_in = rms_scaled(mixed_res, norm_gain_ffn).astype(jnp.bfloat16)
    flat_routes = routes.reshape(-1)
    expert_hits = (
        flat_routes[:, None] == jnp.arange(expert_count, dtype=jnp.int32)[None, :]
    ).astype(jnp.int32)
    earlier = jnp.cumsum(expert_hits, axis=0) - expert_hits
    slot_index = jnp.sum(earlier * expert_hits, axis=1)
    in_slot = (slot_index[:, None] == jnp.arange(slot_count, dtype=jnp.int32)[None, :]).astype(
        jnp.float32
    )
    placing = expert_hits.astype(jnp.float32)[:, :, None] * in_slot[:, None, :]
    placing = placing.reshape(row_count, TOP, expert_count * slot_count)
    selector = jnp.sum(placing, axis=1).astype(jnp.bfloat16)
    weighing = jnp.sum(placing * route_weights[:, :, None], axis=1)
    packed = jnp.einsum("ra,rd->ad", selector, ffn_in, preferred_element_type=jnp.float32).astype(
        jnp.bfloat16
    )
    outgoing = jnp.broadcast_to(
        packed.reshape(expert_count, 1, slot_count, model_width),
        (expert_count, SPAN, slot_count, model_width),
    )
    outgoing = outgoing.reshape(expert_count * SPAN, slot_count, model_width)
    arrived = lax.all_to_all(outgoing, "ep", split_axis=0, concat_axis=0, tiled=True)
    sources, slots, width = arrived.shape
    flat_rows = arrived.reshape(sources * slots, width)
    gate_part = jnp.dot(flat_rows, expert_gate, preferred_element_type=jnp.float32)
    up_part = jnp.dot(flat_rows, expert_up, preferred_element_type=jnp.float32)
    hidden = (jax.nn.silu(gate_part) * up_part).astype(jnp.bfloat16)
    expert_part = jnp.dot(hidden, expert_down, preferred_element_type=jnp.float32)
    col_share = lax.psum_scatter(
        expert_part.astype(jnp.bfloat16), "tp", scatter_dimension=1, tiled=True
    ).astype(jnp.float32)
    returned = lax.all_to_all(
        col_share.reshape(sources, slots, -1).astype(jnp.bfloat16),
        "ep",
        split_axis=0,
        concat_axis=0,
        tiled=True,
    ).astype(jnp.float32)
    col_width = returned.shape[2]
    per_expert = jnp.sum(returned.reshape(expert_count, SPAN, slot_count, col_width), axis=1)
    per_expert = per_expert.reshape(expert_count * slot_count, col_width)
    routed = jnp.dot(
        weighing, per_expert, precision=lax.Precision.HIGHEST, preferred_element_type=jnp.float32
    )
    col_start = lax.axis_index("tp") * col_width
    residual_cols = lax.dynamic_slice_in_dim(mixed_res, col_start, col_width, 1)
    layer_out = (residual_cols + routed).astype(jnp.bfloat16)
    return (layer_out, new_keys, new_values, new_log_gate)


def solution(mesh):
    placed = (
        P("ep", None),
        P(),
        P("ep", "tp"),
        P("ep", "tp"),
        P("ep", "tp"),
        P(None, "tp"),
        P("tp"),
        P("ep", "tp", None),
        P("ep", "tp", None),
        P("ep", "tp", None),
        P("ep"),
        P("tp", None),
        P(),
        P(),
        P(None, ("ep", "tp")),
        P(None, ("ep", "tp")),
        P(("ep", "tp"), None),
        P("ep", None),
        P("ep", None),
    )
    return jax.shard_map(
        body,
        mesh=mesh,
        in_specs=placed,
        out_specs=(P("ep", "tp"), P("ep", "tp"), P("ep", "tp"), P("ep", "tp")),
        check_vma=False,
    )
```
